32 devices in a mesh: grp: 2 (over x), sp: 4 (over z), tp: 4 (over y, core).
Axes of the slice: x: 2, y: 2, z: 4, core: 2. Of those that a mesh axis runs over, the one named last changes fastest.
Arguments:
- tokens: bfloat16 [1792, 4096], P(('grp', 'sp'), 'tp'), parts along dimension 0, may hold values from -130 to 130
- rms_gain: float32 [2, 4096], replicated, may hold values from 0.1 to 1.9
- w_value: bfloat16 [2, 4096, 2048], P(None, 'sp', 'tp'), may hold values from -0.09375 to 0.09375
- w_gate: bfloat16 [2, 4096, 2048], P(None, 'sp', 'tp'), may hold values from -0.09375 to 0.09375
- taps: float32 [2, 31, 2048], P(None, None, 'tp'), may hold values from -8 to 8
- ln_gain: float32 [2, 2048], P(None, 'tp'), may hold values from 0.1 to 1.9
- ln_bias: float32 [2, 2048], P(None, 'tp'), may hold values from -3 to 3
- w_out: bfloat16 [2, 2048, 4096], P(None, 'sp', 'tp'), may hold values from -0.125 to 0.125
Outputs:
- result: bfloat16 [1792, 4096], P(('grp', 'sp'), 'tp'), parts along dimension 0
The draws below stay inside these ranges and needn't reach their ends.
There are 2 independent parts, one for each index of `grp`. The reference program is written for one: setup_inputs(seed, part) draws one part's arguments, and reference() takes and returns one part's arrays. A program takes and returns all parts, laid end to end along the dimension named above; an argument that names none is the same for every part. Nothing has to cross between parts.
All inputs are finite; a program needn't handle non-finite values.
Results may differ from the reference program's by a relative error of at most 0.009.
Values may be sent and summed in bfloat16 or wider, within the bound.
A program may use at most 64 MiB of HBM per device.

```python
import jax
import jax.numpy as jnp
from jax import lax

D = 4096
CH = 2048
WIDTH = 31
LAYERS = 2
TOKENS = 896


def draw_tokens(key, part):
    keys = jax.random.split(jax.random.fold_in(key, 11), 3)
    column = jnp.arange(D, dtype=jnp.float32) / D
    col_scale = jnp.exp(jnp.log(4.0) * column + jax.random.uniform(keys[1], (D,), jnp.float32, -0.4, 0.4))
    row_scale = jnp.exp(jax.random.uniform(keys[2], (TOKENS, 1), jnp.float32, jnp.log(0.5), jnp.log(5.0)))
    base = jax.random.truncated_normal(keys[0], -4.0, 4.0, (TOKENS, D), jnp.float32)
    return (base * col_scale[None, :] * row_scale).astype(jnp.bfloat16)


def draw_taps(key, part):
    keys = jax.random.split(jax.random.fold_in(key, 23), 2)
    channel = jnp.arange(CH, dtype=jnp.float32) / CH
    scale = jnp.exp(jnp.log(10.0) * channel[None, None, :] + jax.random.uniform(keys[1], (LAYERS, 1, CH), jnp.float32, -0.3, 0.3)) / jnp.sqrt(1.0 * WIDTH)
    base = jax.random.truncated_normal(keys[0], -3.0, 3.0, (LAYERS, WIDTH, CH), jnp.float32)
    return base * scale


def level_of(key, shape, cuts, least, top_value):
    def one(dim, parts):
        draws = jax.random.uniform(jax.random.fold_in(jax.random.fold_in(key, 6), dim), (parts,), jnp.float32, least / len(cuts), top_value / len(cuts))
        return jnp.repeat(jnp.exp(draws), shape[dim] // parts).reshape((-1,) + (1,) * (len(shape) - dim - 1))

    loudness = one(*cuts[0])
    for cut in cuts[1:]:
        loudness = loudness * one(*cut)
    return loudness


def scatter_about(own_key, shape, width, reach, shards=(), kind=jnp.bfloat16):
    array = width * jax.random.normal(own_key, shape, jnp.float32)
    if shards:
        array = array * level_of(own_key, shape, shards, -0.22, 0.18)
    return jnp.clip(array, -reach, reach).astype(kind)


def setup_inputs(seed: int = 0, part: int = 0) -> dict:
    arg_keys = jax.random.split(jax.random.key(seed), 9)
    part_keys = jax.random.split(jax.random.fold_in(arg_keys[8], part), 9)
    tokens = draw_tokens(jax.random.fold_in(jax.random.fold_in(arg_keys[8], part), 71), part)
    rms_gain = jnp.clip(1.0 + 0.18 * jax.random.normal(arg_keys[1], (LAYERS, D), jnp.float32), 0.1, 1.9)
    w_value = scatter_about(arg_keys[2], (LAYERS, D, CH), D ** -0.5, 0.09375, ((1, 4), (2, 4)))
    w_gate = scatter_about(arg_keys[3], (LAYERS, D, CH), D ** -0.5, 0.09375, ((1, 4), (2, 4)))
    taps = draw_taps(jax.random.fold_in(arg_keys[8], 71), part)
    ln_gain = jnp.clip(1.0 + 0.18 * jax.random.normal(arg_keys[5], (LAYERS, CH), jnp.float32), 0.1, 1.9)
    ln_bias = scatter_about(arg_keys[6], (LAYERS, CH), 0.5, 3.0, ((1, 4),), jnp.float32)
    w_out = scatter_about(arg_keys[7], (LAYERS, CH, D), CH ** -0.5, 0.125, ((1, 4), (2, 4)))
    return dict(tokens=tokens, rms_gain=rms_gain, w_value=w_value, w_gate=w_gate, taps=taps, ln_gain=ln_gain, ln_bias=ln_bias, w_out=w_out)


def reference(tokens, rms_gain, w_value, w_gate, taps, ln_gain, ln_bias, w_out):
    hidden = tokens
    for layer in range(LAYERS):
        wide = hidden.astype(jnp.float32)
        normed = (wide * lax.rsqrt(lax.optimization_barrier(jnp.mean(wide * wide, axis=1, keepdims=True)) + 1e-06) * rms_gain[layer]).astype(jnp.bfloat16)
        value = jnp.dot(normed, w_value[layer], preferred_element_type=jnp.float32)
        gate = jnp.dot(normed, w_gate[layer], preferred_element_type=jnp.float32)
        glu = (value * jax.nn.sigmoid(gate)).astype(jnp.bfloat16)
        padded = jnp.concatenate([jnp.zeros((WIDTH - 1, CH), jnp.bfloat16), glu], axis=0).astype(jnp.float32)
        conv = jnp.zeros((TOKENS, CH), jnp.float32)
        for k in range(WIDTH):
            conv = conv + taps[layer, k][None, :] * padded[k:k + TOKENS]
        mean = lax.optimization_barrier(jnp.mean(conv, axis=1, keepdims=True))
        var = lax.optimization_barrier(jnp.mean(conv * conv, axis=1, keepdims=True)) - mean * mean
        normed_conv = (conv - mean) * lax.rsqrt(var + 1e-05) * ln_gain[layer] + ln_bias[layer]
        act = jax.nn.silu(normed_conv).astype(jnp.bfloat16)
        branch = jnp.dot(act, w_out[layer], preferred_element_type=jnp.float32)
        hidden = (hidden.astype(jnp.float32) + branch).astype(jnp.bfloat16)
    return hidden
```

```python
import functools

import jax
import jax.numpy as jnp
from jax import lax
from jax.experimental import pallas as pl
from jax.experimental.pallas import tpu as pltpu
from jax.sharding import PartitionSpec as P

LANES = 128
BF16, F32 = jnp.bfloat16, jnp.float32
CUTS = 4


def passed_along(block, axis, distance):
    devices = range(lax.axis_size(axis))
    route = [(i - distance, i) for i in devices if i - distance in devices]
    return lax.ppermute(block, axis, route)


def norm_rows(wide, gain):
    return (wide * lax.rsqrt(jnp.mean(wide * wide, axis=1, keepdims=True) + 1e-06) * gain).astype(
        jnp.bfloat16
    )


def to_depth(rows):
    return lax.all_to_all(rows, "sp", split_axis=1, concat_axis=0, tiled=True)


def summed(partial):
    sp = lax.axis_size("sp")
    rows = partial.shape[0] // sp
    parts = partial.astype(jnp.bfloat16).reshape(sp, rows, partial.shape[1])
    parts = lax.all_to_all(parts, "sp", split_axis=0, concat_axis=0, tiled=True)
    return jnp.sum(parts.astype(jnp.float32), axis=0)


def send(src, dst, send_sem, recv_sem, **where):
    return pltpu.make_async_remote_copy(
        src_ref=src,
        dst_ref=dst,
        send_sem=send_sem,
        recv_sem=recv_sem,
        device_id=where,
        device_id_type=pl.DeviceIdType.MESH,
    )


def gated_conv(
    layers, sp, tp,
    h_hbm, gain_hbm, wv_hbm, wg_hbm, taps_hbm, lng_hbm, lnb_hbm, wo_hbm, out_ref,
    h_ref, gain_ref, taps_ref, lng_ref, lnb_ref, mid,
    wv, wg, wo, pieces, spread, xs, going, coming, own, sq, sq_sum, stat,
    halo_out, halo_in, ext, conv, acts,
    i_sem, w_sem, a_send, a_recv, b_send, c_send, c_relay, x_recv, r_send, r_recv,
    q_send, q_recv, s_send, s_recv, h_send, h_recv, g_send, g_relay, g_recv,
    o_sem, z_send, z_recv, y_send, y_recv,
):
    s, c, g = lax.axis_index("sp"), lax.axis_index("tp"), lax.axis_index("grp")
    grp, share = wo.shape[2], wo.shape[3]
    padded = sq.shape[3]
    rows, depth = h_ref.shape
    chans = taps_ref.shape[2]
    part = depth // tp
    step = going.shape[-1]
    chunks = chans // step
    pairs = tp // 2
    sibling = c + 1 - 2 * (c % 2)
    reach = taps_ref.shape[0]
    pad = halo_in.shape[1]
    cuts = z_recv.shape[2]
    early = cuts // 2
    cut = share // cuts

    first_loads = [
        pltpu.make_async_copy(h_hbm, h_ref, i_sem.at[0]),
        pltpu.make_async_copy(
            gain_hbm.at[:, pl.ds(pl.multiple_of(c * depth, LANES), depth)], gain_ref, i_sem.at[1]
        ),
    ]
    small_loads = [
        pltpu.make_async_copy(taps_hbm, taps_ref, i_sem.at[2]),
        pltpu.make_async_copy(lng_hbm, lng_ref, i_sem.at[3]),
        pltpu.make_async_copy(lnb_hbm, lnb_ref, i_sem.at[4]),
    ]
    in_loads = [
        (
            pltpu.make_async_copy(wv_hbm.at[l], wv.at[l], w_sem.at[l, 0]),
            pltpu.make_async_copy(wg_hbm.at[l], wg.at[l], w_sem.at[l, 1]),
        )
        for l in range(layers)
    ]
    out_loads = [
        [
            pltpu.make_async_copy(
                wo_hbm.at[l, pl.ds(n * share, share)], wo.at[l, s, n], o_sem.at[l, n]
            )
            for n in range(grp)
        ]
        for l in range(layers)
    ]
    for load in first_loads:
        load.start()
    for l in range(layers):
        for load in out_loads[l]:
            load.start()
        for load in in_loads[l]:
            load.start()
    for load in small_loads:
        load.start()

    barrier = pltpu.get_barrier_semaphore()
    for j in range(1, tp):
        pl.semaphore_signal(
            barrier, inc=1, device_id={"tp": (c + j) % tp}, device_id_type=pl.DeviceIdType.MESH
        )
    for j in range(1, sp):
        pl.semaphore_signal(
            barrier, inc=1, device_id={"sp": (s + j) % sp}, device_id_type=pl.DeviceIdType.MESH
        )
    for j in range(1, grp):
        pl.semaphore_signal(
            barrier, inc=1, device_id={"grp": (g + j) % grp}, device_id_type=pl.DeviceIdType.MESH
        )

    def to_row(column):
        column = jnp.concatenate([column, jnp.zeros((padded - rows, LANES), F32)], axis=0)
        return jnp.sum(column.T, axis=0, keepdims=True)

    def to_column(row):
        return jnp.broadcast_to(row, (LANES, padded)).T[:rows, 0:1]

    def turn(i):
        return ((c // 2 + 1 + i // 2) % pairs) * 2 + (c + 1 + i) % 2

    def a_copy(l, to, frm):
        return send(
            pieces.at[l, to], spread.at[l, frm], a_send.at[l, to], a_recv.at[l, frm], tp=to
        )

    def q_copy(l, to, frm):
        return send(sq.at[l, frm], sq.at[l, frm], q_send.at[l, to], q_recv.at[l, frm], tp=to)

    def prepare(l, p, block):
        wide = block.astype(F32)
        total = sq_sum[...]
        for lane in range(0, part, LANES):
            tile = wide[:, lane : lane + LANES]
            total = total + tile * tile
        sq_sum[...] = total
        gain = gain_ref[l : l + 1, pl.ds(pl.multiple_of(p * part, LANES), part)]
        pieces[l, p] = (wide * gain).astype(BF16)

    def hand_out(l, p):
        @pl.when(p != c)
        def _():
            a_copy(l, p, c).start()

        @pl.when(p == c)
        def _():
            spread[l, c] = pieces[l, c]

    def hand_out_squares(l):
        sq[l, c] = jnp.broadcast_to(to_row(sq_sum[...]), sq.shape[2:])
        for j in range(1, tp):
            q_copy(l, (c + j) % tp, c).start()

    def beyond(left):
        return (1 - left) * (sp - 1 - s) + left * s

    def z_copy(l, left, o, k):
        rows_k = pl.ds(k * cut, cut)
        return send(
            wo.at[l, o, g, rows_k],
            wo.at[l, o, g, rows_k],
            z_send.at[l, left, o, k],
            z_recv.at[l, o, k],
            sp=s + 1 - 2 * left,
        )

    def y_copy(l, j, o, n, k):
        rows_k = pl.ds(k * cut, cut)
        return send(
            wo.at[l, o, n, rows_k],
            wo.at[l, o, n, rows_k],
            y_send.at[l, j, o, k],
            y_recv.at[l, o, n, k],
            grp=(g + j) % grp,
        )

    def z_own(l, left, k):
        @pl.when(beyond(left) > 0)
        def _():
            z_copy(l, left, s, k).start()

    def z_pass(l, left, i, k):
        o = s + (2 * left - 1) * i

        @pl.when((o >= 0) & (o < sp))
        def _():
            rows_k = pl.ds(k * cut, cut)
            send(
                wo.at[l, o, g, rows_k],
                wo.at[l, o, g, rows_k],
                z_send.at[l, left, o, k],
                z_recv.at[l, o, k],
                sp=(s + 1) % sp,
            ).wait_recv()

            @pl.when(beyond(left) > 0)
            def _():
                z_copy(l, left, o, k).start()

            for j in range(1, grp):
                y_copy(l, j, o, g, k).start()

    def z_rest(l, lean):
        for left in range(2):

            @pl.when((beyond(left) <= 1) == lean)
            def _():
                for k in range(early if l == 0 else cuts, cuts):
                    z_own(l, left, k)
                for k in range(early):
                    z_pass(l, left, 1, k)

    def place(j):
        left = (j + 2 * s // sp) % 2
        k = j // 2
        d = (1 - left) * (sp - 1 - k) + left * k
        return left, d, (1 - 2 * left) * (d - s) > 0

    def each(body):
        def one(j, carry):
            left, d, valid = place(j)

            @pl.when(valid)
            def _():
                body(j, left, d)

            return carry

        lax.fori_loop(0, 2 * (sp - 1), one, 0)

    def upstream(left):
        return (1 - left) * s + left * (sp - 1 - s) > 0

    def b_copy(l, to, frm):
        return send(
            spread.at[l, to], xs.at[l, c, frm], b_send.at[l, to], x_recv.at[l, c, frm], sp=to
        )

    def c_copy(l, to, d, sem):
        return send(xs.at[l, c, d], xs.at[l, c, d], sem, x_recv.at[l, c, d], tp=to)

    def relay(l, p, d):
        return send(
            xs.at[l, p, d], xs.at[l, p, d], c_relay.at[l, p, d], x_recv.at[l, p, d], tp=sibling
        )

    def r_copy(l, left, d, slot):
        return send(
            going.at[l, left, d, slot],
            coming.at[l, left, d, slot],
            r_send.at[l, left, d, slot],
            r_recv.at[l, left, d, slot],
            sp=s + 1 - 2 * left,
        )

    def h_copy(l, to):
        return send(halo_out.at[l], halo_in.at[l], h_send.at[l], h_recv.at[l], sp=to)

    def s_copy(l, to, frm):
        return send(stat.at[l, frm], stat.at[l, frm], s_send.at[l, to], s_recv.at[l, frm], tp=to)

    def g_copy(l, to, p, sem):
        return send(acts.at[l, p], acts.at[l, p], sem, g_recv.at[l, p], tp=to)

    def layer_of(l):
        def held(e):
            @pl.when(e != c)
            def _():
                a_copy(l, c, e).wait_recv()

        def scatter(j, left, d):
            held(d)
            b_copy(l, d, s).start()

        each(scatter)
        held(s)
        xs[l, c, s] = spread[l, s]

        def gather(d):
            @pl.when(d != s)
            def _():
                relay(l, c, d).wait_recv()

            for j in range(1, pairs):
                c_copy(l, (c + 2 * j) % tp, d, c_send.at[l, j, d]).start()
            c_copy(l, sibling, d, c_send.at[l, 0, d]).start()

        gather(s)
        each(lambda j, left, d: gather(d))
        z_rest(l, True)
        for load in in_loads[l]:
            load.wait()

        def ready(d):
            for j in range(1, pairs):
                p = (c + 2 * j) % tp
                relay(l, p, d).wait_recv()
                relay(l, p, d).start()
            for j in range(pairs):
                relay(l, (sibling + 2 * j) % tp, d).wait_recv()

        def product(d, weight, at):
            acc = jnp.zeros((rows, step), F32)
            for p in range(tp):
                acc = acc + jnp.dot(
                    xs[l, p, d],
                    weight[l, p * part : (p + 1) * part, pl.ds(at, step)],
                    preferred_element_type=F32,
                )
            return acc

        def r_arrived(left, d, slot):
            send(
                going.at[l, left, d, slot],
                coming.at[l, left, d, slot],
                r_send.at[l, left, d, slot],
                r_recv.at[l, left, d, slot],
                sp=(s + 1) % sp,
            ).wait_recv()

        def partial(j, left, d):
            ready(d)
            for half, weight in enumerate((wv, wg)):

                def one(i, carry):
                    slot = half * chunks + i
                    own[half] = product(d, weight, pl.multiple_of(i * step, step))

                    @pl.when(upstream(left))
                    def _():
                        r_arrived(left, d, slot)
                        own[half] += coming[l, left, d, slot].astype(F32)

                    going[l, left, d, slot] = own[half].astype(BF16)
                    r_copy(l, left, d, slot).start()
                    return carry

                lax.fori_loop(0, chunks, one, 0)

        each(partial)
        z_rest(l, False)
        ready(s)
        for j in range(1, tp):
            q_copy(l, c, (c + j) % tp).wait_recv()
        squares = sq[l, 0]
        for p in range(1, tp):
            squares = squares + sq[l, p]
        scale = to_column(lax.rsqrt(squares[0:1] / (depth * tp) + 1e-06))

        def finish(i, carry):
            at = pl.multiple_of(i * step, step)
            for half, weight in enumerate((wv, wg)):
                slot = half * chunks + i
                own[half] = product(s, weight, at)
                for left in range(2):

                    @pl.when(upstream(left))
                    def _():
                        r_arrived(left, s, slot)
                        own[half] += coming[l, left, s, slot].astype(F32)

            glu = (own[0] * scale * jax.nn.sigmoid(own[1] * scale)).astype(BF16)
            ext[pad:, pl.ds(at, step)] = glu.astype(F32)
            halo_out[l, :, pl.ds(at, step)] = glu[rows - pad :]
            return carry

        lax.fori_loop(0, chunks, finish, 0)

        @pl.when(s < sp - 1)
        def _():
            h_copy(l, s + 1).start()

        for k in range(early, cuts):
            for left in range(2):
                z_pass(l, left, 1, k)

        @pl.when(s > 0)
        def _():
            h_copy(l, (s + 1) % sp).wait_recv()
            ext[:pad] = halo_in[l].astype(F32)

        @pl.when(s == 0)
        def _():
            ext[:pad] = jnp.zeros((pad, chans), F32)

        if l == 0:
            for load in small_loads:
                load.wait()
        first = pad - (reach - 1)

        def convolve(i, carry):
            lanes = pl.ds(pl.multiple_of(i * LANES, LANES), LANES)
            acc = jnp.zeros((rows, LANES), F32)
            for k in range(reach):
                acc = acc + taps_ref[k, l : l + 1, lanes] * ext[first + k : first + k + rows, lanes]
            conv[:, lanes] = acc
            return carry

        lax.fori_loop(0, chans // LANES, convolve, 0)
        total = jnp.zeros((rows, LANES), F32)
        total_sq = jnp.zeros((rows, LANES), F32)
        for at in range(0, chans, LANES):
            tile = conv[:, at : at + LANES]
            total = total + tile
            total_sq = total_sq + tile * tile
        half = sq.shape[2] // 2
        stat[l, c] = jnp.concatenate(
            [jnp.broadcast_to(to_row(t), (half, padded)) for t in (total, total_sq)], axis=0
        )
        for j in range(1, tp):
            s_copy(l, (c + j) % tp, c).start()
        for k in range(early):
            for left in range(2):
                z_pass(l, left, 2, k)
        for j in range(1, tp):
            s_copy(l, c, (c + j) % tp).wait_recv()
        stats = stat[l, 0]
        for p in range(1, tp):
            stats = stats + stat[l, p]
        mean = stats[0:1] / (chans * tp)
        var = stats[half : half + 1] / (chans * tp) - mean * mean
        inv = to_column(lax.rsqrt(var + 1e-05))
        mean = to_column(mean)
        for at in range(0, chans, LANES):
            lanes = slice(at, at + LANES)
            shaped = (conv[:, lanes] - mean) * inv * lng_ref[l : l + 1, lanes] + lnb_ref[
                l : l + 1, lanes
            ]
            acts[l, c, :, lanes] = (shaped / (1.0 + jnp.exp(-shaped))).astype(BF16)

        for j in range(1, pairs):
            g_copy(l, (c + 2 * j) % tp, c, g_send.at[l, j]).start()
        g_copy(l, sibling, c, g_send.at[l, 0]).start()
        for j in range(1, pairs):
            p = (c + 2 * j) % tp
            g_copy(l, sibling, p, g_relay.at[l, p]).wait_recv()
            g_copy(l, sibling, p, g_relay.at[l, p]).start()
        for k in range(early, cuts):
            for left in range(2):
                z_pass(l, left, 2, k)
        for i in range(3, sp):
            for k in range(cuts):
                for left in range(2):
                    z_pass(l, left, i, k)
        if l + 1 < layers:
            for load in out_loads[l + 1]:
                load.wait()
            for k in range(cuts):
                for left in range(2):
                    z_own(l + 1, left, k)
        for j in range(pairs):
            p = (sibling + 2 * j) % tp
            g_copy(l, sibling, p, g_relay.at[l, p]).wait_recv()
        for i in range(1, sp):
            for left in range(2):
                o = s + (2 * left - 1) * i

                @pl.when((o >= 0) & (o < sp))
                def _():
                    for k in range(cuts):
                        for j in range(1, grp):
                            y_copy(l, j, o, (g + j) % grp, k).wait_recv()

        sq_sum[...] = jnp.zeros_like(sq_sum)

        def project(i, carry):
            p = turn(i)
            lanes = pl.ds(pl.multiple_of(p * part, LANES), part)
            acc = jnp.zeros((rows, part), F32)
            for e in range(tp):
                for n in range(grp):
                    acc = acc + jnp.dot(
                        acts[l, e, :, n * share : (n + 1) * share],
                        wo[l, e, n, :, lanes],
                        preferred_element_type=F32,
                    )
            before = h_ref if l == 0 else mid.at[l - 1]
            block = (before[:, lanes].astype(F32) + acc).astype(BF16)
            if l + 1 < layers:
                mid[l, :, lanes] = block
                prepare(l + 1, p, block)
                hand_out(l + 1, p)
            else:
                out_ref[:, lanes] = block
            return carry

        lax.fori_loop(0, tp, project, 0)
        if l + 1 < layers:
            hand_out_squares(l + 1)

    sq_sum[...] = jnp.zeros_like(sq_sum)
    for load in first_loads:
        load.wait()
    for p in range(tp):
        prepare(0, p, h_ref[:, p * part : (p + 1) * part])
    for load in out_loads[0]:
        load.wait()
    pl.semaphore_wait(barrier, tp + sp + grp - 3)

    def first_hand_out(i, carry):
        hand_out(0, turn(i))
        return carry

    lax.fori_loop(0, tp, first_hand_out, 0)
    for k in range(early):
        for left in range(2):
            z_own(0, left, k)
    hand_out_squares(0)
    for l in range(layers):
        layer_of(l)

    for l in range(layers):
        for j in range(1, tp):
            a_copy(l, (c + j) % tp, c).wait_send()
            q_copy(l, (c + j) % tp, c).wait_send()
            s_copy(l, (c + j) % tp, c).wait_send()
        for j in range(1, sp):
            b_copy(l, (s + j) % sp, s).wait_send()

        def sent(d, carry):
            c_copy(l, sibling, d, c_send.at[l, 0, d]).wait_send()
            for j in range(1, pairs):
                p = (c + 2 * j) % tp
                c_copy(l, p, d, c_send.at[l, j, d]).wait_send()
                relay(l, p, d).wait_send()
            return carry

        lax.fori_loop(0, sp, sent, 0)

        def partial_sent(j, left, d):
            def one(slot, carry):
                r_copy(l, left, d, slot).wait_send()
                return carry

            lax.fori_loop(0, 2 * chunks, one, 0)

        each(partial_sent)

        @pl.when(s < sp - 1)
        def _():
            h_copy(l, s + 1).wait_send()

        for i in range(sp):
            for left in range(2):
                o = s + (2 * left - 1) * i

                @pl.when((o >= 0) & (o < sp))
                def _():
                    for k in range(cuts):

                        @pl.when(beyond(left) > 0)
                        def _():
                            z_copy(l, left, o, k).wait_send()

                        if i > 0:
                            for j in range(1, grp):
                                y_copy(l, j, o, g, k).wait_send()

        g_copy(l, sibling, c, g_send.at[l, 0]).wait_send()
        for j in range(1, pairs):
            p = (c + 2 * j) % tp
            g_copy(l, p, c, g_send.at[l, j]).wait_send()
            g_copy(l, sibling, p, g_relay.at[l, p]).wait_send()


def fused(tokens, rms_gain, w_value, w_gate, taps, ln_gain, ln_bias, w_out):
    sp, tp, grp = (lax.axis_size(a) for a in ("sp", "tp", "grp"))
    rows, depth = tokens.shape
    padded = -(-rows // LANES) * LANES
    layers, chans, reach = w_value.shape[0], w_value.shape[2], taps.shape[1]
    part, step = depth // tp, min(2 * LANES, chans)
    slots = 2 * (chans // step)
    pad = -(-(reach - 1) // 16) * 16
    share = w_out.shape[1] // grp
    cuts = CUTS
    vmem, dma = pltpu.VMEM, pltpu.SemaphoreType.DMA
    there = pl.BlockSpec(memory_space=pltpu.HBM)
    return pl.pallas_call(
        functools.partial(gated_conv, layers, sp, tp),
        out_shape=jax.ShapeDtypeStruct((rows, depth), BF16),
        in_specs=[there] * 8,
        out_specs=pl.BlockSpec(memory_space=pltpu.VMEM),
        scratch_shapes=[
            vmem((rows, depth), BF16),
            vmem((layers, depth), F32),
            vmem((reach, layers, chans), F32),
            vmem((layers, chans), F32),
            vmem((layers, chans), F32),
            vmem((layers, rows, depth), BF16),
            vmem((layers, depth, chans), BF16),
            vmem((layers, depth, chans), BF16),
            vmem((layers, sp, grp, share, depth), BF16),
            vmem((layers, tp, rows, part), BF16),
            vmem((layers, tp, rows, part), BF16),
            vmem((layers, tp, sp, rows, part), BF16),
            vmem((layers, 2, sp, slots, rows, step), BF16),
            vmem((layers, 2, sp, slots, rows, step), BF16),
            vmem((2, rows, step), F32),
            vmem((layers, tp, 8, padded), F32),
            vmem((rows, LANES), F32),
            vmem((layers, tp, 8, padded), F32),
            vmem((layers, pad, chans), BF16),
            vmem((layers, pad, chans), BF16),
            vmem((pad + rows, chans), F32),
            vmem((rows, chans), F32),
            vmem((layers, tp, rows, chans), BF16),
            dma((5,)), dma((layers, 2)),
            dma((layers, tp)), dma((layers, tp)), dma((layers, sp)),
            dma((layers, tp, sp)), dma((layers, tp, sp)), dma((layers, tp, sp)),
            dma((layers, 2, sp, slots)), dma((layers, 2, sp, slots)),
            dma((layers, tp)), dma((layers, tp)), dma((layers, tp)), dma((layers, tp)),
            dma((layers,)), dma((layers,)),
            dma((layers, tp)), dma((layers, tp)), dma((layers, tp)),
            dma((layers, grp)), dma((layers, 2, sp, cuts)), dma((layers, sp, cuts)),
            dma((layers, grp, sp, cuts)), dma((layers, sp, grp, cuts)),
        ],
        compiler_params=pltpu.CompilerParams(
            collective_id=0, has_side_effects=True, vmem_limit_bytes=60 * 2**20
        ),
    )(
        tokens, rms_gain, w_value, w_gate, jnp.transpose(taps, (1, 0, 2)), ln_gain, ln_bias, w_out
    )


def fits(tokens, w_value, taps, w_out):
    sp, tp, grp = (lax.axis_size(a) for a in ("sp", "tp", "grp"))
    rows, depth = tokens.shape
    chans = w_value.shape[2]
    return (
        sp == tp
        and tp % 2 == 0
        and depth % (tp * LANES) == 0
        and chans % (LANES * grp) == 0
        and w_out.shape[1] % (16 * grp * CUTS) == 0
        and w_out.shape[1] == chans
        and chans % min(2 * LANES, chans) == 0
        and rows % 16 == 0
        and rows >= -(-(taps.shape[1] - 1) // 16) * 16
    )


def shards(tokens, rms_gain, w_value, w_gate, taps, ln_gain, ln_bias, w_out):
    if fits(tokens, w_value, taps, w_out):
        return fused(tokens, rms_gain, w_value, w_gate, taps, ln_gain, ln_bias, w_out)
    layers = w_value.shape[0]
    tok_rows = tokens.shape[0]
    chans = w_value.shape[2]
    all_chans = chans * lax.axis_size("tp")
    reach = taps.shape[1]
    current = tokens
    for layer in range(layers):
        whole_rows = lax.all_gather(current, "tp", axis=1, tiled=True)
        normed = to_depth(norm_rows(whole_rows.astype(jnp.float32), rms_gain[layer]))
        both = jnp.concatenate([w_value[layer], w_gate[layer]], axis=1)
        both = summed(jnp.dot(normed, both, preferred_element_type=jnp.float32))
        glu = (both[:, :chans] * jax.nn.sigmoid(both[:, chans:])).astype(jnp.bfloat16)
        earlier = passed_along(glu[tok_rows - (reach - 1) :], "sp", 1)
        extended = jnp.concatenate([earlier, glu], axis=0).astype(jnp.float32)
        conv = jnp.zeros((tok_rows, chans), jnp.float32)
        for k in range(reach):
            conv = conv + taps[layer, k][None, :] * extended[k : k + tok_rows]
        total, total_sq = lax.psum((jnp.sum(conv, axis=1), jnp.sum(conv * conv, axis=1)), "tp")
        mean = total / all_chans
        var = total_sq / all_chans - mean * mean
        shaped = (conv - mean[:, None]) * lax.rsqrt(var + 1e-05)[:, None] * ln_gain[layer][
            None, :
        ] + ln_bias[layer][None, :]
        act = jax.nn.silu(shaped).astype(jnp.bfloat16)
        act_all = to_depth(lax.all_gather(act, "tp", axis=1, tiled=True))
        branch = summed(jnp.dot(act_all, w_out[layer], preferred_element_type=jnp.float32))
        current = (current.astype(jnp.float32) + branch).astype(jnp.bfloat16)
    return current


def solution(mesh):
    return jax.shard_map(
        shards,
        mesh=mesh,
        in_specs=(
            P(("grp", "sp"), "tp"),
            P(),
            P(None, "sp", "tp"),
            P(None, "sp", "tp"),
            P(None, None, "tp"),
            P(None, "tp"),
            P(None, "tp"),
            P(None, "sp", "tp"),
        ),
        out_specs=P(("grp", "sp"), "tp"),
        check_vma=False,
    )
```

```python
import functools

import jax
import jax.numpy as jnp
from jax import lax
from jax.experimental import pallas as pl
from jax.experimental.pallas import tpu as pltpu
from jax.sharding import PartitionSpec as P

LANES = 128
BF16, F32 = jnp.bfloat16, jnp.float32
CUTS = 4


def passed_along(block, axis, distance):
    devices = range(lax.axis_size(axis))
    route = [(i - distance, i) for i in devices if i - distance in devices]
    return lax.ppermute(block, axis, route)


def norm_rows(wide, gain):
    return (wide * lax.rsqrt(jnp.mean(wide * wide, axis=1, keepdims=True) + 1e-06) * gain).astype(
        jnp.bfloat16
    )


def to_depth(rows):
    return lax.all_to_all(rows, "sp", split_axis=1, concat_axis=0, tiled=True)


def summed(partial):
    sp = lax.axis_size("sp")
    rows = partial.shape[0] // sp
    parts = partial.astype(jnp.bfloat16).reshape(sp, rows, partial.shape[1])
    parts = lax.all_to_all(parts, "sp", split_axis=0, concat_axis=0, tiled=True)
    return jnp.sum(parts.astype(jnp.float32), axis=0)


def send(src, dst, send_sem, recv_sem, **where):
    return pltpu.make_async_remote_copy(
        src_ref=src,
        dst_ref=dst,
        send_sem=send_sem,
        recv_sem=recv_sem,
        device_id=where,
        device_id_type=pl.DeviceIdType.MESH,
    )


def gated_conv(
    layers, sp, tp,
    h_hbm, gain_hbm, wv_hbm, wg_hbm, taps_hbm, lng_hbm, lnb_hbm, wo_hbm, out_ref,
    h_ref, gain_ref, taps_ref, lng_ref, lnb_ref, mid,
    wv, wg, wo, pieces, spread, xs, going, coming, own, sq, sq_sum, stat,
    halo_out, halo_in, ext, conv, acts,
    i_sem, w_sem, a_send, a_recv, b_send, c_send, c_relay, x_recv, r_send, r_recv,
    q_send, q_recv, s_send, s_recv, h_send, h_recv, g_send, g_relay, g_recv,
    o_sem, z_send, z_recv, y_send, y_recv,
):
    s, c, g = lax.axis_index("sp"), lax.axis_index("tp"), lax.axis_index("grp")
    grp, share = wo.shape[2], wo.shape[3]
    padded = sq.shape[3]
    rows, depth = h_ref.shape
    chans = taps_ref.shape[2]
    part = depth // tp
    step = going.shape[-1]
    chunks = chans // step
    pairs = tp // 2
    sibling = c + 1 - 2 * (c % 2)
    reach = taps_ref.shape[0]
    pad = halo_in.shape[2]
    cuts = z_recv.shape[2]
    early = cuts // 2
    cut = share // cuts

    first_loads = [
        pltpu.make_async_copy(h_hbm, h_ref, i_sem.at[0]),
        pltpu.make_async_copy(
            gain_hbm.at[:, pl.ds(pl.multiple_of(c * depth, LANES), depth)], gain_ref, i_sem.at[1]
        ),
    ]
    small_loads = [
        pltpu.make_async_copy(taps_hbm, taps_ref, i_sem.at[2]),
        pltpu.make_async_copy(lng_hbm, lng_ref, i_sem.at[3]),
        pltpu.make_async_copy(lnb_hbm, lnb_ref, i_sem.at[4]),
    ]
    in_loads = [
        (
            pltpu.make_async_copy(wv_hbm.at[l], wv.at[l], w_sem.at[l, 0]),
            pltpu.make_async_copy(wg_hbm.at[l], wg.at[l], w_sem.at[l, 1]),
        )
        for l in range(layers)
    ]
    out_loads = [
        [
            pltpu.make_async_copy(
                wo_hbm.at[l, pl.ds(n * share, share)], wo.at[l, s, n], o_sem.at[l, n]
            )
            for n in range(grp)
        ]
        for l in range(layers)
    ]
    for load in first_loads:
        load.start()
    for l in range(layers):
        for load in out_loads[l]:
            load.start()
        for load in in_loads[l]:
            load.start()
    for load in small_loads:
        load.start()

    barrier = pltpu.get_barrier_semaphore()
    for j in range(1, tp):
        pl.semaphore_signal(
            barrier, inc=1, device_id={"tp": (c + j) % tp}, device_id_type=pl.DeviceIdType.MESH
        )
    for j in range(1, sp):
        pl.semaphore_signal(
            barrier, inc=1, device_id={"sp": (s + j) % sp}, device_id_type=pl.DeviceIdType.MESH
        )
    for j in range(1, grp):
        pl.semaphore_signal(
            barrier, inc=1, device_id={"grp": (g + j) % grp}, device_id_type=pl.DeviceIdType.MESH
        )

    def to_row(column):
        column = jnp.concatenate([column, jnp.zeros((padded - rows, LANES), F32)], axis=0)
        return jnp.sum(column.T, axis=0, keepdims=True)

    def to_column(row):
        return jnp.broadcast_to(row, (LANES, padded)).T[:rows, 0:1]

    def turn(i):
        return ((c // 2 + 1 + i // 2) % pairs) * 2 + (c + 1 + i) % 2

    def a_copy(l, to, frm):
        return send(
            pieces.at[l, to], spread.at[l, frm], a_send.at[l, to], a_recv.at[l, frm], tp=to
        )

    def q_copy(l, to, frm):
        return send(sq.at[l, frm], sq.at[l, frm], q_send.at[l, to], q_recv.at[l, frm], tp=to)

    def prepare(l, p, block):
        wide = block.astype(F32)
        total = sq_sum[...]
        for lane in range(0, part, LANES):
            tile = wide[:, lane : lane + LANES]
            total = total + tile * tile
        sq_sum[...] = total
        gain = gain_ref[l : l + 1, pl.ds(pl.multiple_of(p * part, LANES), part)]
        pieces[l, p] = (wide * gain).astype(BF16)

    def hand_out(l, p):
        @pl.when(p != c)
        def _():
            a_copy(l, p, c).start()

        @pl.when(p == c)
        def _():
            spread[l, c] = pieces[l, c]

    def hand_out_squares(l):
        sq[l, c] = jnp.broadcast_to(to_row(sq_sum[...]), sq.shape[2:])
        for j in range(1, tp):
            q_copy(l, (c + j) % tp, c).start()

    def beyond(left):
        return (1 - left) * (sp - 1 - s) + left * s

    def z_copy(l, left, o, k):
        rows_k = pl.ds(k * cut, cut)
        return send(
            wo.at[l, o, g, rows_k],
            wo.at[l, o, g, rows_k],
            z_send.at[l, left, o, k],
            z_recv.at[l, o, k],
            sp=s + 1 - 2 * left,
        )

    def y_copy(l, j, o, n, k):
        rows_k = pl.ds(k * cut, cut)
        return send(
            wo.at[l, o, n, rows_k],
            wo.at[l, o, n, rows_k],
            y_send.at[l, j, o, k],
            y_recv.at[l, o, n, k],
            grp=(g + j) % grp,
        )

    def z_pass(l, left, i, k):
        o = s + (2 * left - 1) * i

        @pl.when((o >= 0) & (o < sp))
        def _():
            rows_k = pl.ds(k * cut, cut)
            send(
                wo.at[l, o, g, rows_k],
                wo.at[l, o, g, rows_k],
                z_send.at[l, left, o, k],
                z_recv.at[l, o, k],
                sp=(s + 1) % sp,
            ).wait_recv()

            @pl.when(beyond(left) > 0)
            def _():
                z_copy(l, left, o, k).start()

            for j in range(1, grp):
                y_copy(l, j, o, g, k).start()

    def moment(l, ahead, i, k):
        if l == 0:
            table = {
                (1, 0): ("start", "start", "gathered", "gathered"),
                (2, 0): ("start", "start", "turned", "turned"),
                (3, 0): ("start", "start", "finished", "finished"),
                (0, 1): ("gathered", "gathered", "summed", "summed"),
                (1, 1): ("gathered", "gathered", "summed", "summed"),
                (2, 1): ("summed", "finished", "counted", "counted"),
                (0, 2): ("summed", "summed", "counted", "counted"),
                (1, 2): ("finished", "counted", "closed", "closed"),
            }
        else:
            table = {
                (1, 0): ("start", "start", "start", "start"),
                (2, 0): ("start", "start", "start", "start"),
                (3, 0): ("tail", "tail", "tail", "tail"),
                (0, 1): ("gathered", "gathered", "gathered", "gathered"),
                (1, 1): ("before", "before", "gathered", "gathered"),
                (2, 1): ("before", "before", "turned", "turned"),
                (0, 2): ("summed", "summed", "summed", "summed"),
                (1, 2): ("summed", "summed", "finished", "finished"),
            }
        return table.get((ahead, i), ("closed",) * 4)[4 * k // cuts]

    def fill(l, point):
        for left in range(2):
            for ahead in range(sp):
                steps = [
                    (i, k)
                    for i in range(sp - ahead)
                    for k in range(cuts)
                    if moment(l, min(ahead, 3), i, k) == point
                ]

                if steps:

                    @pl.when(beyond(left) == ahead)
                    def _():
                        for i, k in steps:
                            if i > 0:
                                z_pass(l, left, i, k)
                            elif ahead > 0:
                                z_copy(l, left, s, k).start()

    def place(j):
        left = (j + 2 * s // sp) % 2
        k = j // 2
        d = (1 - left) * (sp - 1 - k) + left * k
        return left, d, (1 - 2 * left) * (d - s) > 0

    def each(body):
        def one(j, carry):
            left, d, valid = place(j)

            @pl.when(valid)
            def _():
                body(j, left, d)

            return carry

        lax.fori_loop(0, 2 * (sp - 1), one, 0)

    def upstream(left):
        return (1 - left) * s + left * (sp - 1 - s) > 0

    def b_copy(l, to, frm):
        return send(
            spread.at[l, to], xs.at[l, c, frm], b_send.at[l, to], x_recv.at[l, c, frm], sp=to
        )

    def c_copy(l, to, d, sem):
        return send(xs.at[l, c, d], xs.at[l, c, d], sem, x_recv.at[l, c, d], tp=to)

    def relay(l, p, d):
        return send(
            xs.at[l, p, d], xs.at[l, p, d], c_relay.at[l, p, d], x_recv.at[l, p, d], tp=sibling
        )

    def r_copy(l, left, d, slot):
        return send(
            going.at[l, left, d, slot],
            coming.at[l, left, d, slot],
            r_send.at[l, left, d, slot],
            r_recv.at[l, left, d, slot],
            sp=s + 1 - 2 * left,
        )

    def h_copy(l, to, i):
        return send(
            halo_out.at[l, i], halo_in.at[l, i], h_send.at[l, i], h_recv.at[l, i], sp=to
        )

    def s_copy(l, to, frm):
        return send(stat.at[l, frm], stat.at[l, frm], s_send.at[l, to], s_recv.at[l, frm], tp=to)

    def g_copy(l, to, p, sem):
        return send(acts.at[l, p], acts.at[l, p], sem, g_recv.at[l, p], tp=to)

    def layer_of(l):
        def held(e):
            @pl.when(e != c)
            def _():
                a_copy(l, c, e).wait_recv()

        def scatter(j, left, d):
            held(d)
            b_copy(l, d, s).start()

        if l > 0:
            fill(l, "before")
        each(scatter)
        held(s)
        xs[l, c, s] = spread[l, s]

        def gather(d):
            @pl.when(d != s)
            def _():
                relay(l, c, d).wait_recv()

            for j in range(1, pairs):
                c_copy(l, (c + 2 * j) % tp, d, c_send.at[l, j, d]).start()
            c_copy(l, sibling, d, c_send.at[l, 0, d]).start()

        gather(s)
        each(lambda j, left, d: gather(d))
        fill(l, "gathered")
        for load in in_loads[l]:
            load.wait()

        def ready(d):
            for j in range(1, pairs):
                p = (c + 2 * j) % tp
                relay(l, p, d).wait_recv()
                relay(l, p, d).start()
            for j in range(pairs):
                relay(l, (sibling + 2 * j) % tp, d).wait_recv()

        def product(d, weight, at):
            acc = jnp.zeros((rows, step), F32)
            for p in range(tp):
                acc = acc + jnp.dot(
                    xs[l, p, d],
                    weight[l, p * part : (p + 1) * part, pl.ds(at, step)],
                    preferred_element_type=F32,
                )
            return acc

        def r_arrived(left, d, slot):
            send(
                going.at[l, left, d, slot],
                coming.at[l, left, d, slot],
                r_send.at[l, left, d, slot],
                r_recv.at[l, left, d, slot],
                sp=(s + 1) % sp,
            ).wait_recv()

        def partial(j, left, d):
            ready(d)
            def one(i, carry):
                for half, weight in enumerate((wv, wg)):
                    slot = 2 * i + half
                    own[half] = product(d, weight, pl.multiple_of(i * step, step))

                    @pl.when(upstream(left))
                    def _():
                        r_arrived(left, d, slot)
                        own[half] += coming[l, left, d, slot].astype(F32)

                    going[l, left, d, slot] = own[half].astype(BF16)
                    r_copy(l, left, d, slot).start()
                return carry

            lax.fori_loop(0, chunks, one, 0)

            @pl.when(j == 0)
            def _():
                fill(l, "turned")

        each(partial)
        fill(l, "summed")
        ready(s)
        for j in range(1, tp):
            q_copy(l, c, (c + j) % tp).wait_recv()
        squares = sq[l, 0]
        for p in range(1, tp):
            squares = squares + sq[l, p]
        scale = to_column(lax.rsqrt(squares[0:1] / (depth * tp) + 1e-06))

        def finish(i, carry):
            at = pl.multiple_of(i * step, step)
            for half, weight in enumerate((wv, wg)):
                slot = 2 * i + half
                own[half] = product(s, weight, at)
                for left in range(2):

                    @pl.when(upstream(left))
                    def _():
                        r_arrived(left, s, slot)
                        own[half] += coming[l, left, s, slot].astype(F32)

            glu = (own[0] * scale * jax.nn.sigmoid(own[1] * scale)).astype(BF16)
            ext[pad:, pl.ds(at, step)] = glu.astype(F32)
            halo_out[l, i] = glu[rows - pad :]

            @pl.when(s < sp - 1)
            def _():
                h_copy(l, s + 1, i).start()

            return carry

        lax.fori_loop(0, chunks, finish, 0)
        if l == 0:
            for load in small_loads:
                load.wait()
        fill(l, "finished")
        first = pad - (reach - 1)

        def convolve(i, carry):
            at = pl.multiple_of(i * step, step)

            @pl.when(s > 0)
            def _():
                h_copy(l, (s + 1) % sp, i).wait_recv()
                ext[:pad, pl.ds(at, step)] = halo_in[l, i].astype(F32)

            @pl.when(s == 0)
            def _():
                ext[:pad, pl.ds(at, step)] = jnp.zeros((pad, step), F32)

            lax.fori_loop(0, step // LANES, functools.partial(strip, at), 0)
            return carry

        def strip(start, i, carry):
            lanes = pl.ds(pl.multiple_of(start + i * LANES, LANES), LANES)
            acc = jnp.zeros((rows, LANES), F32)
            for k in range(reach):
                acc = acc + taps_ref[k, l : l + 1, lanes] * ext[first + k : first + k + rows, lanes]
            conv[:, lanes] = acc
            return carry

        lax.fori_loop(0, chunks, convolve, 0)
        total = jnp.zeros((rows, LANES), F32)
        total_sq = jnp.zeros((rows, LANES), F32)
        for at in range(0, chans, LANES):
            tile = conv[:, at : at + LANES]
            total = total + tile
            total_sq = total_sq + tile * tile
        half = sq.shape[2] // 2
        stat[l, c] = jnp.concatenate(
            [jnp.broadcast_to(to_row(t), (half, padded)) for t in (total, total_sq)], axis=0
        )
        for j in range(1, tp):
            s_copy(l, (c + j) % tp, c).start()
        fill(l, "counted")
        if l + 1 < layers:
            for load in out_loads[l + 1]:
                load.wait()
            fill(l + 1, "tail")
        for j in range(1, tp):
            s_copy(l, c, (c + j) % tp).wait_recv()
        stats = stat[l, 0]
        for p in range(1, tp):
            stats = stats + stat[l, p]
        mean = stats[0:1] / (chans * tp)
        var = stats[half : half + 1] / (chans * tp) - mean * mean
        inv = to_column(lax.rsqrt(var + 1e-05))
        mean = to_column(mean)
        for at in range(0, chans, LANES):
            lanes = slice(at, at + LANES)
            shaped = (conv[:, lanes] - mean) * inv * lng_ref[l : l + 1, lanes] + lnb_ref[
                l : l + 1, lanes
            ]
            acts[l, c, :, lanes] = (shaped / (1.0 + jnp.exp(-shaped))).astype(BF16)

        for j in range(1, pairs):
            g_copy(l, (c + 2 * j) % tp, c, g_send.at[l, j]).start()
        g_copy(l, sibling, c, g_send.at[l, 0]).start()
        fill(l, "closed")
        if l + 1 < layers:
            fill(l + 1, "start")
        for j in range(1, pairs):
            p = (c + 2 * j) % tp
            g_copy(l, sibling, p, g_relay.at[l, p]).wait_recv()
            g_copy(l, sibling, p, g_relay.at[l, p]).start()
        for j in range(pairs):
            p = (sibling + 2 * j) % tp
            g_copy(l, sibling, p, g_relay.at[l, p]).wait_recv()
        for i in range(1, sp):
            for left in range(2):
                o = s + (2 * left - 1) * i

                @pl.when((o >= 0) & (o < sp))
                def _():
                    for k in range(cuts):
                        for j in range(1, grp):
                            y_copy(l, j, o, (g + j) % grp, k).wait_recv()

        sq_sum[...] = jnp.zeros_like(sq_sum)

        def project(i, carry):
            p = turn(i)
            lanes = pl.ds(pl.multiple_of(p * part, LANES), part)
            acc = jnp.zeros((rows, part), F32)
            for e in range(tp):
                for n in range(grp):
                    acc = acc + jnp.dot(
                        acts[l, e, :, n * share : (n + 1) * share],
                        wo[l, e, n, :, lanes],
                        preferred_element_type=F32,
                    )
            before = h_ref if l == 0 else mid.at[l - 1]
            block = (before[:, lanes].astype(F32) + acc).astype(BF16)
            if l + 1 < layers:
                mid[l, :, lanes] = block
                prepare(l + 1, p, block)
                hand_out(l + 1, p)
            else:
                out_ref[:, lanes] = block
            return carry

        lax.fori_loop(0, tp, project, 0)
        if l + 1 < layers:
            hand_out_squares(l + 1)

    sq_sum[...] = jnp.zeros_like(sq_sum)
    for load in first_loads:
        load.wait()
    for p in range(tp):
        prepare(0, p, h_ref[:, p * part : (p + 1) * part])
    for load in out_loads[0]:
        load.wait()
    pl.semaphore_wait(barrier, tp + sp + grp - 3)

    def first_hand_out(i, carry):
        hand_out(0, turn(i))
        return carry

    lax.fori_loop(0, tp, first_hand_out, 0)
    fill(0, "start")
    hand_out_squares(0)
    for l in range(layers):
        layer_of(l)

    for l in range(layers):
        for j in range(1, tp):
            a_copy(l, (c + j) % tp, c).wait_send()
            q_copy(l, (c + j) % tp, c).wait_send()
            s_copy(l, (c + j) % tp, c).wait_send()
        for j in range(1, sp):
            b_copy(l, (s + j) % sp, s).wait_send()

        def sent(d, carry):
            c_copy(l, sibling, d, c_send.at[l, 0, d]).wait_send()
            for j in range(1, pairs):
                p = (c + 2 * j) % tp
                c_copy(l, p, d, c_send.at[l, j, d]).wait_send()
                relay(l, p, d).wait_send()
            return carry

        lax.fori_loop(0, sp, sent, 0)

        def partial_sent(j, left, d):
            def one(slot, carry):
                r_copy(l, left, d, slot).wait_send()
                return carry

            lax.fori_loop(0, 2 * chunks, one, 0)

        each(partial_sent)

        @pl.when(s < sp - 1)
        def _():
            for i in range(chunks):
                h_copy(l, s + 1, i).wait_send()

        for i in range(sp):
            for left in range(2):
                o = s + (2 * left - 1) * i

                @pl.when((o >= 0) & (o < sp))
                def _():
                    for k in range(cuts):

                        @pl.when(beyond(left) > 0)
                        def _():
                            z_copy(l, left, o, k).wait_send()

                        if i > 0:
                            for j in range(1, grp):
                                y_copy(l, j, o, g, k).wait_send()

        g_copy(l, sibling, c, g_send.at[l, 0]).wait_send()
        for j in range(1, pairs):
            p = (c + 2 * j) % tp
            g_copy(l, p, c, g_send.at[l, j]).wait_send()
            g_copy(l, sibling, p, g_relay.at[l, p]).wait_send()


def fused(tokens, rms_gain, w_value, w_gate, taps, ln_gain, ln_bias, w_out):
    sp, tp, grp = (lax.axis_size(a) for a in ("sp", "tp", "grp"))
    rows, depth = tokens.shape
    padded = -(-rows // LANES) * LANES
    layers, chans, reach = w_value.shape[0], w_value.shape[2], taps.shape[1]
    part, step = depth // tp, min(2 * LANES, chans)
    slots = 2 * (chans // step)
    pad = -(-(reach - 1) // 16) * 16
    share = w_out.shape[1] // grp
    cuts = CUTS
    vmem, dma = pltpu.VMEM, pltpu.SemaphoreType.DMA
    there = pl.BlockSpec(memory_space=pltpu.HBM)
    return pl.pallas_call(
        functools.partial(gated_conv, layers, sp, tp),
        out_shape=jax.ShapeDtypeStruct((rows, depth), BF16),
        in_specs=[there] * 8,
        out_specs=pl.BlockSpec(memory_space=pltpu.VMEM),
        scratch_shapes=[
            vmem((rows, depth), BF16),
            vmem((layers, depth), F32),
            vmem((reach, layers, chans), F32),
            vmem((layers, chans), F32),
            vmem((layers, chans), F32),
            vmem((layers, rows, depth), BF16),
            vmem((layers, depth, chans), BF16),
            vmem((layers, depth, chans), BF16),
            vmem((layers, sp, grp, share, depth), BF16),
            vmem((layers, tp, rows, part), BF16),
            vmem((layers, tp, rows, part), BF16),
            vmem((layers, tp, sp, rows, part), BF16),
            vmem((layers, 2, sp, slots, rows, step), BF16),
            vmem((layers, 2, sp, slots, rows, step), BF16),
            vmem((2, rows, step), F32),
            vmem((layers, tp, 8, padded), F32),
            vmem((rows, LANES), F32),
            vmem((layers, tp, 8, padded), F32),
            vmem((layers, chans // step, pad, step), BF16),
            vmem((layers, chans // step, pad, step), BF16),
            vmem((pad + rows, chans), F32),
            vmem((rows, chans), F32),
            vmem((layers, tp, rows, chans), BF16),
            dma((5,)), dma((layers, 2)),
            dma((layers, tp)), dma((layers, tp)), dma((layers, sp)),
            dma((layers, tp, sp)), dma((layers, tp, sp)), dma((layers, tp, sp)),
            dma((layers, 2, sp, slots)), dma((layers, 2, sp, slots)),
            dma((layers, tp)), dma((layers, tp)), dma((layers, tp)), dma((layers, tp)),
            dma((layers, chans // step)), dma((layers, chans // step)),
            dma((layers, tp)), dma((layers, tp)), dma((layers, tp)),
            dma((layers, grp)), dma((layers, 2, sp, cuts)), dma((layers, sp, cuts)),
            dma((layers, grp, sp, cuts)), dma((layers, sp, grp, cuts)),
        ],
        compiler_params=pltpu.CompilerParams(
            collective_id=0, has_side_effects=True, vmem_limit_bytes=60 * 2**20
        ),
    )(
        tokens, rms_gain, w_value, w_gate, jnp.transpose(taps, (1, 0, 2)), ln_gain, ln_bias, w_out
    )


def fits(tokens, w_value, taps, w_out):
    sp, tp, grp = (lax.axis_size(a) for a in ("sp", "tp", "grp"))
    rows, depth = tokens.shape
    chans = w_value.shape[2]
    return (
        sp == tp
        and tp % 2 == 0
        and depth % (tp * LANES) == 0
        and chans % (LANES * grp) == 0
        and w_out.shape[1] % (16 * grp * CUTS) == 0
        and w_out.shape[1] == chans
        and chans % min(2 * LANES, chans) == 0
        and rows % 16 == 0
        and rows >= -(-(taps.shape[1] - 1) // 16) * 16
    )


def shards(tokens, rms_gain, w_value, w_gate, taps, ln_gain, ln_bias, w_out):
    if fits(tokens, w_value, taps, w_out):
        return fused(tokens, rms_gain, w_value, w_gate, taps, ln_gain, ln_bias, w_out)
    layers = w_value.shape[0]
    tok_rows = tokens.shape[0]
    chans = w_value.shape[2]
    all_chans = chans * lax.axis_size("tp")
    reach = taps.shape[1]
    current = tokens
    for layer in range(layers):
        whole_rows = lax.all_gather(current, "tp", axis=1, tiled=True)
        normed = to_depth(norm_rows(whole_rows.astype(jnp.float32), rms_gain[layer]))
        both = jnp.concatenate([w_value[layer], w_gate[layer]], axis=1)
        both = summed(jnp.dot(normed, both, preferred_element_type=jnp.float32))
        glu = (both[:, :chans] * jax.nn.sigmoid(both[:, chans:])).astype(jnp.bfloat16)
        earlier = passed_along(glu[tok_rows - (reach - 1) :], "sp", 1)
        extended = jnp.concatenate([earlier, glu], axis=0).astype(jnp.float32)
        conv = jnp.zeros((tok_rows, chans), jnp.float32)
        for k in range(reach):
            conv = conv + taps[layer, k][None, :] * extended[k : k + tok_rows]
        total, total_sq = lax.psum((jnp.sum(conv, axis=1), jnp.sum(conv * conv, axis=1)), "tp")
        mean = total / all_chans
        var = total_sq / all_chans - mean * mean
        shaped = (conv - mean[:, None]) * lax.rsqrt(var + 1e-05)[:, None] * ln_gain[layer][
            None, :
        ] + ln_bias[layer][None, :]
        act = jax.nn.silu(shaped).astype(jnp.bfloat16)
        act_all = to_depth(lax.all_gather(act, "tp", axis=1, tiled=True))
        branch = summed(jnp.dot(act_all, w_out[layer], preferred_element_type=jnp.float32))
        current = (current.astype(jnp.float32) + branch).astype(jnp.bfloat16)
    return current


def solution(mesh):
    return jax.shard_map(
        shards,
        mesh=mesh,
        in_specs=(
            P(("grp", "sp"), "tp"),
            P(),
            P(None, "sp", "tp"),
            P(None, "sp", "tp"),
            P(None, None, "tp"),
            P(None, "tp"),
            P(None, "tp"),
            P(None, "sp", "tp"),
        ),
        out_specs=P(("grp", "sp"), "tp"),
        check_vma=False,
    )
```

```python
import functools

import jax
import jax.numpy as jnp
from jax import lax
from jax.experimental import pallas as pl
from jax.experimental.pallas import tpu as pltpu
from jax.sharding import PartitionSpec as P

LANES = 128
BF16, F32 = jnp.bfloat16, jnp.float32
LOTS = 2
CUTS = 4

FIRST = {
    (1, 0): ("start", "start", "gathered", "gathered"),
    (2, 0): ("start", "start", "scattered", "turned"),
    (3, 0): ("start", "start", "scattered", "finished"),
    (0, 1): ("gathered", "gathered", "summed", "summed"),
    (1, 1): ("gathered", "gathered", "summed", "summed"),
    (2, 1): ("gathered summed", "gathered finished", "gathered finished", "counted"),
    (0, 2): ("summed", "summed", "counted", "counted"),
    (1, 2): ("counted", "counted", "closed", "closed"),
}
LATER = {
    (1, 0): ("start", "start", "start", "start"),
    (2, 0): ("tail", "tail", "tail", "tail"),
    (3, 0): ("tail", "tail", "tail", "tail"),
    (0, 1): ("gathered", "gathered", "gathered", "gathered"),
    (1, 1): ("gathered", "gathered", "gathered", "gathered"),
    (2, 1): ("start", "before", "scattered", "finished"),
    (0, 2): ("summed", "summed", "summed", "summed"),
    (1, 2): ("summed", "summed", "counted", "counted"),
}


def passed_along(block, axis, distance):
    devices = range(lax.axis_size(axis))
    route = [(i - distance, i) for i in devices if i - distance in devices]
    return lax.ppermute(block, axis, route)


def norm_rows(wide, gain):
    return (wide * lax.rsqrt(jnp.mean(wide * wide, axis=1, keepdims=True) + 1e-06) * gain).astype(
        jnp.bfloat16
    )


def to_depth(rows):
    return lax.all_to_all(rows, "sp", split_axis=1, concat_axis=0, tiled=True)


def summed(partial):
    sp = lax.axis_size("sp")
    rows = partial.shape[0] // sp
    parts = partial.astype(jnp.bfloat16).reshape(sp, rows, partial.shape[1])
    parts = lax.all_to_all(parts, "sp", split_axis=0, concat_axis=0, tiled=True)
    return jnp.sum(parts.astype(jnp.float32), axis=0)


def send(src, dst, send_sem, recv_sem, **where):
    return pltpu.make_async_remote_copy(
        src_ref=src,
        dst_ref=dst,
        send_sem=send_sem,
        recv_sem=recv_sem,
        device_id=where,
        device_id_type=pl.DeviceIdType.MESH,
    )


def gated_conv(
    layers, sp, tp,
    h_hbm, gain_hbm, wv_hbm, wg_hbm, taps_hbm, lng_hbm, lnb_hbm, wo_hbm, out_ref,
    h_ref, gain_ref, taps_ref, lng_ref, lnb_ref, mid,
    wvg, wo, lent, pieces, spread, xs, going, coming, own, sq, sq_sum, stat,
    halo_out, halo_in, ext, conv, acts,
    i_sem, w_sem, a_send, a_recv, b_send, c_send, c_relay, x_recv, r_send, r_recv,
    q_send, q_recv, s_send, s_recv, h_send, h_recv, g_send, g_relay, g_recv,
    o_sem, z_send, z_recv, y_send, y_recv, v_send, v_recv, u_send, u_recv,
):
    s, c, g = lax.axis_index("sp"), lax.axis_index("tp"), lax.axis_index("grp")
    grp, share = wo.shape[2], wo.shape[3]
    padded = sq.shape[3]
    rows, depth = h_ref.shape
    chans = taps_ref.shape[2]
    part = depth // tp
    step = going.shape[-1]
    chunks = chans // step
    pairs = tp // 2
    sibling = c + 1 - 2 * (c % 2)
    reach = taps_ref.shape[0]
    pad = halo_in.shape[2]
    cuts = z_recv.shape[2]
    early = cuts // 2
    cut = share // cuts
    lots = v_recv.shape[2]
    lot = depth // (grp * lots)
    early_lots = 2 * lots
    kept = chunks - lent.shape[3] // step
    at_end = (s == 0) | (s == sp - 1)
    at_host = (s == 1) | (s == sp - 2)
    partner = (s == 0) + (sp - 2) * (s == sp - 1) + (sp - 1) * (s == sp - 2)

    first_loads = [
        pltpu.make_async_copy(h_hbm, h_ref, i_sem.at[0]),
        pltpu.make_async_copy(
            gain_hbm.at[:, pl.ds(pl.multiple_of(c * depth, LANES), depth)], gain_ref, i_sem.at[1]
        ),
    ]
    small_loads = [
        pltpu.make_async_copy(taps_hbm, taps_ref, i_sem.at[2]),
        pltpu.make_async_copy(lng_hbm, lng_ref, i_sem.at[3]),
        pltpu.make_async_copy(lnb_hbm, lnb_ref, i_sem.at[4]),
    ]
    in_loads = [
        (
            pltpu.make_async_copy(wv_hbm.at[l], wvg.at[l, 0], w_sem.at[l, 0]),
            pltpu.make_async_copy(wg_hbm.at[l], wvg.at[l, 1], w_sem.at[l, 1]),
        )
        for l in range(layers)
    ]
    out_loads = [
        [
            pltpu.make_async_copy(
                wo_hbm.at[l, pl.ds(n * share, share)], wo.at[l, s, n], o_sem.at[l, n]
            )
            for n in range(grp)
        ]
        for l in range(layers)
    ]
    for load in first_loads:
        load.start()
    for l in range(layers):
        for load in out_loads[l]:
            load.start()
        for load in in_loads[l]:
            load.start()
    for load in small_loads:
        load.start()

    barrier = pltpu.get_barrier_semaphore()
    for j in range(1, tp):
        pl.semaphore_signal(
            barrier, inc=1, device_id={"tp": (c + j) % tp}, device_id_type=pl.DeviceIdType.MESH
        )
    for j in range(1, sp):
        pl.semaphore_signal(
            barrier, inc=1, device_id={"sp": (s + j) % sp}, device_id_type=pl.DeviceIdType.MESH
        )
    for j in range(1, grp):
        pl.semaphore_signal(
            barrier, inc=1, device_id={"grp": (g + j) % grp}, device_id_type=pl.DeviceIdType.MESH
        )

    def to_row(column):
        column = jnp.concatenate([column, jnp.zeros((padded - rows, LANES), F32)], axis=0)
        return jnp.sum(column.T, axis=0, keepdims=True)

    def to_column(row):
        return jnp.broadcast_to(row, (LANES, padded)).T[:rows, 0:1]

    def turn(i):
        return ((c // 2 + 1 + i // 2) % pairs) * 2 + (c + 1 + i) % 2

    def a_copy(l, to, frm):
        return send(
            pieces.at[l, to], spread.at[l, frm], a_send.at[l, to], a_recv.at[l, frm], tp=to
        )

    def q_copy(l, to, frm):
        return send(sq.at[l, frm], sq.at[l, frm], q_send.at[l, to], q_recv.at[l, frm], tp=to)

    def prepare(l, p, block):
        wide = block.astype(F32)
        total = sq_sum[...]
        for lane in range(0, part, LANES):
            tile = wide[:, lane : lane + LANES]
            total = total + tile * tile
        sq_sum[...] = total
        gain = gain_ref[l : l + 1, pl.ds(pl.multiple_of(p * part, LANES), part)]
        pieces[l, p] = (wide * gain).astype(BF16)

    def hand_out(l, p):
        @pl.when(p != c)
        def _():
            a_copy(l, p, c).start()

        @pl.when(p == c)
        def _():
            spread[l, c] = pieces[l, c]

    def hand_out_squares(l):
        sq[l, c] = jnp.broadcast_to(to_row(sq_sum[...]), sq.shape[2:])
        for j in range(1, tp):
            q_copy(l, (c + j) % tp, c).start()

    def beyond(left):
        return (1 - left) * (sp - 1 - s) + left * s

    def z_copy(l, left, o, k):
        rows_k = pl.ds(k * cut, cut)
        return send(
            wo.at[l, o, g, rows_k],
            wo.at[l, o, g, rows_k],
            z_send.at[l, left, o, k],
            z_recv.at[l, o, k],
            sp=s + 1 - 2 * left,
        )

    def y_copy(l, j, o, n, k):
        rows_k = pl.ds(k * cut, cut)
        return send(
            wo.at[l, o, n, rows_k],
            wo.at[l, o, n, rows_k],
            y_send.at[l, j, o, k],
            y_recv.at[l, o, n, k],
            grp=(g + j) % grp,
        )

    def z_take(l, o, k):
        rows_k = pl.ds(k * cut, cut)
        send(
            wo.at[l, o, g, rows_k],
            wo.at[l, o, g, rows_k],
            z_send.at[l, 0, o, k],
            z_recv.at[l, o, k],
            sp=(s + 1) % sp,
        ).wait_recv()
        for j in range(1, grp):
            y_copy(l, j, o, g, k).start()

    def moment(l, ahead, i, k):
        if l == 0:
            table = FIRST
        else:
            table = LATER
        points = table.get((ahead, i), ("closed",) * 4)[4 * k // cuts]
        return points.split() if " " in points else (points, points)

    def fill(l, point):
        for left in range(2):
            for ahead in range(sp):
                steps = []
                for i in range(sp - ahead):
                    for k in range(cuts):
                        taken, sent_on = moment(l, min(ahead, 3), i, k)
                        if i > 0 and taken == point:
                            steps.append((i, k, True))
                        if ahead > 0 and sent_on == point:
                            steps.append((i, k, False))

                if steps:

                    @pl.when(beyond(left) == ahead)
                    def _():
                        for i, k, take in steps:
                            o = s + (2 * left - 1) * i
                            if take:
                                z_take(l, o, k)
                            else:
                                z_copy(l, left, o, k).start()

    def lends(l):
        return l > 0 and sp >= 4 and kept < chunks

    def sent_chunks(l, d):
        if not lends(l):
            return chunks
        return chunks - (chunks - kept) * (at_end & (d == partner)).astype(jnp.int32)

    def v_copy(l, t):
        half, q = t % 2, t // 2
        rows_q = pl.ds(pl.multiple_of((g * lots + q) * lot, lot), lot)
        return send(
            wvg.at[l, half, rows_q, pl.ds(kept * step, (chunks - kept) * step)],
            lent.at[l - 1, half, rows_q],
            v_send.at[l - 1, half, q],
            v_recv.at[l - 1, half, q],
            sp=partner,
        )

    def u_copy(l, j, t, n):
        half, q = t % 2, t // 2
        rows_q = pl.ds(pl.multiple_of((n * lots + q) * lot, lot), lot)
        return send(
            lent.at[l - 1, half, rows_q],
            lent.at[l - 1, half, rows_q],
            u_send.at[l - 1, j, half, q],
            u_recv.at[l - 1, half, n, q],
            grp=(g + j) % grp,
        )

    def lend_out(l, first, last):
        if lends(l):

            @pl.when(at_end)
            def _():
                for t in range(first, last):
                    v_copy(l, t).start()

    def lend_in(l, first, last):
        if lends(l):

            @pl.when(at_host)
            def _():
                for t in range(first, last):
                    v_copy(l, t).wait_recv()
                    for j in range(1, grp):
                        u_copy(l, j, t, g).start()

    def place(j):
        left = (j + 2 * s // sp) % 2
        k = j // 2
        d = (1 - left) * (sp - 1 - k) + left * k
        return left, d, (1 - 2 * left) * (d - s) > 0

    def each(body):
        def one(j, carry):
            left, d, valid = place(j)

            @pl.when(valid)
            def _():
                body(j, left, d)

            return carry

        lax.fori_loop(0, 2 * (sp - 1), one, 0)

    def behind(left):
        return (1 - left) * s + left * (sp - 1 - s)

    def upstream(left):
        return behind(left) > 0

    def b_copy(l, to, frm):
        return send(
            spread.at[l, to], xs.at[l, c, frm], b_send.at[l, to], x_recv.at[l, c, frm], sp=to
        )

    def c_copy(l, to, d, sem):
        return send(xs.at[l, c, d], xs.at[l, c, d], sem, x_recv.at[l, c, d], tp=to)

    def relay(l, p, d):
        return send(
            xs.at[l, p, d], xs.at[l, p, d], c_relay.at[l, p, d], x_recv.at[l, p, d], tp=sibling
        )

    def r_copy(l, left, d, slot):
        return send(
            going.at[l, left, d, slot],
            coming.at[l, left, d, slot],
            r_send.at[l, left, d, slot],
            r_recv.at[l, left, d, slot],
            sp=s + 1 - 2 * left,
        )

    def h_copy(l, to, i):
        return send(
            halo_out.at[l, i], halo_in.at[l, i], h_send.at[l, i], h_recv.at[l, i], sp=to
        )

    def s_copy(l, to, frm):
        return send(stat.at[l, frm], stat.at[l, frm], s_send.at[l, to], s_recv.at[l, frm], tp=to)

    def g_copy(l, to, p, sem):
        return send(acts.at[l, p], acts.at[l, p], sem, g_recv.at[l, p], tp=to)

    def layer_of(l):
        slots = 2 * chunks
        inner = sp == 4 and slots >= 2
        mids = 1 - at_end.astype(jnp.int32)

        def held(e):
            @pl.when(e != c)
            def _():
                a_copy(l, c, e).wait_recv()

        def scatter(j, left, d):
            held(d)
            b_copy(l, d, s).start()

        if l > 0:
            fill(l, "before")
            lend_in(l, 0, lots)
        each(scatter)
        fill(l, "scattered")
        held(s)
        xs[l, c, s] = spread[l, s]
        if lends(l):

            @pl.when(at_host)
            def _():
                xs[l, c, sp] = spread[l, partner]

        def gather(d, arriving=True):
            if arriving:
                relay(l, c, d).wait_recv()
            for j in range(1, pairs):
                c_copy(l, (c + 2 * j) % tp, d, c_send.at[l, j, d]).start()
            c_copy(l, sibling, d, c_send.at[l, 0, d]).start()

        gather(s, False)
        if inner:
            gather(place(0)[1])
            gather(place(1 + at_end.astype(jnp.int32))[1])
        else:
            each(lambda j, left, d: gather(d))
        if l == 0:
            for load in in_loads[l]:
                load.wait()

        def ready(d):
            for j in range(1, pairs):
                p = (c + 2 * j) % tp
                relay(l, p, d).wait_recv()
                relay(l, p, d).start()
            for j in range(pairs):
                relay(l, (sibling + 2 * j) % tp, d).wait_recv()

        def product(d, weight, at):
            acc = jnp.zeros((rows, step), F32)
            for p in range(tp):
                acc = acc + jnp.dot(
                    xs[l, p, d],
                    weight[p * part : (p + 1) * part, pl.ds(at, step)],
                    preferred_element_type=F32,
                )
            return acc

        def r_arrived(left, d, slot):
            send(
                going.at[l, left, d, slot],
                coming.at[l, left, d, slot],
                r_send.at[l, left, d, slot],
                r_recv.at[l, left, d, slot],
                sp=(s + 1) % sp,
            ).wait_recv()

        def partial(slot, left, d):
            half, i = slot % 2, slot // 2

            @pl.when(slot == 0)
            def _():
                ready(d)

            own[half] = product(d, wvg.at[l, half], pl.multiple_of(i * step, step))

            @pl.when(upstream(left))
            def _():
                r_arrived(left, d, slot)
                own[half] += coming[l, left, d, slot].astype(F32)

            going[l, left, d, slot] = own[half].astype(BF16)
            r_copy(l, left, d, slot).start()

        def turn_slot(t):
            if not inner:
                return t // slots, t % slots
            u = t - 2
            woven = ((u >= 0) & (u < 2 * slots)).astype(jnp.int32)
            aside = woven * (1 - u % 2) * mids
            k = jnp.where(woven == 1, 2 + u // 2, jnp.where(u < 0, t, t - slots))
            k = mids * k + (1 - mids) * t
            j = aside + (1 - aside) * 2 * (k // slots)
            return j, aside * (u // 2) + (1 - aside) * (k % slots)

        def advance(t, carry):
            j, slot = turn_slot(t)
            left, d, valid = place(j)

            @pl.when(valid & (slot < 2 * sent_chunks(l, d)))
            def _():
                partial(slot, left, d)

            @pl.when(t == 0)
            def _():
                if inner:
                    gather(place(2 + 2 * at_end.astype(jnp.int32))[1])
                if lends(l):

                    @pl.when(at_host)
                    def _():
                        gather(sp, False)

                lend_in(l, lots, early_lots)
                fill(l, "gathered")
                lend_out(l, early_lots, 2 * lots)

            @pl.when(t == slots - 1 + (mids * (slots - 2) if inner else 0))
            def _():
                fill(l, "turned")
                lend_in(l, early_lots, 2 * lots)

            @pl.when(t == 2 * slots - 1)
            def _():
                fill(l, "halfway")

            return carry

        lax.fori_loop(0, slots * (3 if inner else 2 * (sp - 1)), advance, 0)
        fill(l, "summed")
        ready(s)
        if lends(l):

            @pl.when(at_host)
            def _():
                ready(sp)
                for t in range(2 * lots):
                    for j in range(1, grp):
                        u_copy(l, j, t, (g + j) % grp).wait_recv()

        for j in range(1, tp):
            q_copy(l, c, (c + j) % tp).wait_recv()
        squares = sq[l, 0]
        for p in range(1, tp):
            squares = squares + sq[l, p]
        scale = to_column(lax.rsqrt(squares[0:1] / (depth * tp) + 1e-06))

        def finish(i, carry):
            at = pl.multiple_of(i * step, step)
            for half in range(2):
                slot = 2 * i + half
                own[half] = product(s, wvg.at[l, half], at)
                if lends(l):

                    @pl.when(at_host & (i >= kept))
                    def _():
                        own[half] += product(
                            sp, lent.at[l - 1, half], pl.multiple_of(at - kept * step, step)
                        )

                for left in range(2):
                    expected = upstream(left)
                    if lends(l):
                        expected = expected & jnp.logical_not(
                            at_host & (behind(left) == 1) & (i >= kept)
                        )

                    @pl.when(expected)
                    def _():
                        r_arrived(left, s, slot)
                        own[half] += coming[l, left, s, slot].astype(F32)

            glu = (own[0] * scale * jax.nn.sigmoid(own[1] * scale)).astype(BF16)
            ext[pad:, pl.ds(at, step)] = glu.astype(F32)
            halo_out[l, i] = glu[rows - pad :]

            @pl.when(s < sp - 1)
            def _():
                h_copy(l, s + 1, i).start()

            return carry

        lax.fori_loop(0, chunks, finish, 0)
        if l == 0:
            for load in small_loads:
                load.wait()
        fill(l, "finished")
        first = pad - (reach - 1)

        def convolve(i, carry):
            at = pl.multiple_of(i * step, step)

            @pl.when(s > 0)
            def _():
                h_copy(l, (s + 1) % sp, i).wait_recv()
                ext[:pad, pl.ds(at, step)] = halo_in[l, i].astype(F32)

            @pl.when(s == 0)
            def _():
                ext[:pad, pl.ds(at, step)] = jnp.zeros((pad, step), F32)

            lax.fori_loop(0, step // LANES, functools.partial(strip, at), 0)
            return carry

        def strip(start, i, carry):
            lanes = pl.ds(pl.multiple_of(start + i * LANES, LANES), LANES)
            acc = jnp.zeros((rows, LANES), F32)
            for k in range(reach):
                acc = acc + taps_ref[k, l : l + 1, lanes] * ext[first + k : first + k + rows, lanes]
            conv[:, lanes] = acc
            return carry

        lax.fori_loop(0, chunks, convolve, 0)
        total = jnp.zeros((rows, LANES), F32)
        total_sq = jnp.zeros((rows, LANES), F32)
        for at in range(0, chans, LANES):
            tile = conv[:, at : at + LANES]
            total = total + tile
            total_sq = total_sq + tile * tile
        half = sq.shape[2] // 2
        stat[l, c] = jnp.concatenate(
            [jnp.broadcast_to(to_row(t), (half, padded)) for t in (total, total_sq)], axis=0
        )
        for j in range(1, tp):
            s_copy(l, (c + j) % tp, c).start()
        fill(l, "counted")
        if l + 1 < layers:
            for load in out_loads[l + 1]:
                load.wait()
            for load in in_loads[l + 1]:
                load.wait()
            fill(l + 1, "tail")
            lend_out(l + 1, 0, early_lots)
        for j in range(1, tp):
            s_copy(l, c, (c + j) % tp).wait_recv()
        stats = stat[l, 0]
        for p in range(1, tp):
            stats = stats + stat[l, p]
        mean = stats[0:1] / (chans * tp)
        var = stats[half : half + 1] / (chans * tp) - mean * mean
        inv = to_column(lax.rsqrt(var + 1e-05))
        mean = to_column(mean)
        for at in range(0, chans, LANES):
            lanes = slice(at, at + LANES)
            shaped = (conv[:, lanes] - mean) * inv * lng_ref[l : l + 1, lanes] + lnb_ref[
                l : l + 1, lanes
            ]
            acts[l, c, :, lanes] = (shaped / (1.0 + jnp.exp(-shaped))).astype(BF16)

        for j in range(1, pairs):
            g_copy(l, (c + 2 * j) % tp, c, g_send.at[l, j]).start()
        g_copy(l, sibling, c, g_send.at[l, 0]).start()
        fill(l, "closed")
        if l + 1 < layers:
            fill(l + 1, "start")
        for j in range(1, pairs):
            p = (c + 2 * j) % tp
            g_copy(l, sibling, p, g_relay.at[l, p]).wait_recv()
            g_copy(l, sibling, p, g_relay.at[l, p]).start()
        for j in range(pairs):
            p = (sibling + 2 * j) % tp
            g_copy(l, sibling, p, g_relay.at[l, p]).wait_recv()
        for i in range(1, sp):
            for left in range(2):
                o = s + (2 * left - 1) * i

                @pl.when((o >= 0) & (o < sp))
                def _():
                    for k in range(cuts):
                        for j in range(1, grp):
                            y_copy(l, j, o, (g + j) % grp, k).wait_recv()

        sq_sum[...] = jnp.zeros_like(sq_sum)

        def project(i, carry):
            p = turn(i)
            lanes = pl.ds(pl.multiple_of(p * part, LANES), part)
            acc = jnp.zeros((rows, part), F32)
            for e in range(tp):
                for n in range(grp):
                    acc = acc + jnp.dot(
                        acts[l, e, :, n * share : (n + 1) * share],
                        wo[l, e, n, :, lanes],
                        preferred_element_type=F32,
                    )
            before = h_ref if l == 0 else mid.at[l - 1]
            block = (before[:, lanes].astype(F32) + acc).astype(BF16)
            if l + 1 < layers:
                mid[l, :, lanes] = block
                prepare(l + 1, p, block)
                hand_out(l + 1, p)
            else:
                out_ref[:, lanes] = block
            return carry

        lax.fori_loop(0, tp, project, 0)
        if l + 1 < layers:
            hand_out_squares(l + 1)

    sq_sum[...] = jnp.zeros_like(sq_sum)
    for load in first_loads:
        load.wait()
    for p in range(tp):
        prepare(0, p, h_ref[:, p * part : (p + 1) * part])
    for load in out_loads[0]:
        load.wait()
    pl.semaphore_wait(barrier, tp + sp + grp - 3)

    def first_hand_out(i, carry):
        hand_out(0, turn(i))
        return carry

    lax.fori_loop(0, tp, first_hand_out, 0)
    fill(0, "start")
    hand_out_squares(0)
    for l in range(layers):
        layer_of(l)

    for l in range(layers):
        for j in range(1, tp):
            a_copy(l, (c + j) % tp, c).wait_send()
            q_copy(l, (c + j) % tp, c).wait_send()
            s_copy(l, (c + j) % tp, c).wait_send()
        each(lambda j, left, d: b_copy(l, d, s).wait_send())

        def sent(d):
            c_copy(l, sibling, d, c_send.at[l, 0, d]).wait_send()
            for j in range(1, pairs):
                p = (c + 2 * j) % tp
                c_copy(l, p, d, c_send.at[l, j, d]).wait_send()
                relay(l, p, d).wait_send()

        sent(s)
        each(lambda j, left, d: sent(d))
        if lends(l):

            @pl.when(at_host)
            def _():
                sent(sp)
                for t in range(2 * lots):
                    for j in range(1, grp):
                        u_copy(l, j, t, g).wait_send()

            @pl.when(at_end)
            def _():
                for t in range(2 * lots):
                    v_copy(l, t).wait_send()


        def partial_sent(j, left, d):
            def one(slot, carry):
                r_copy(l, left, d, slot).wait_send()
                return carry

            lax.fori_loop(0, 2 * sent_chunks(l, d), one, 0)

        each(partial_sent)

        @pl.when(s < sp - 1)
        def _():
            for i in range(chunks):
                h_copy(l, s + 1, i).wait_send()

        for i in range(sp):
            for left in range(2):
                o = s + (2 * left - 1) * i

                @pl.when((o >= 0) & (o < sp))
                def _():
                    for k in range(cuts):

                        @pl.when(beyond(left) > 0)
                        def _():
                            z_copy(l, left, o, k).wait_send()

                        if i > 0:
                            for j in range(1, grp):
                                y_copy(l, j, o, g, k).wait_send()

        g_copy(l, sibling, c, g_send.at[l, 0]).wait_send()
        for j in range(1, pairs):
            p = (c + 2 * j) % tp
            g_copy(l, p, c, g_send.at[l, j]).wait_send()
            g_copy(l, sibling, p, g_relay.at[l, p]).wait_send()


def fused(tokens, rms_gain, w_value, w_gate, taps, ln_gain, ln_bias, w_out):
    sp, tp, grp = (lax.axis_size(a) for a in ("sp", "tp", "grp"))
    rows, depth = tokens.shape
    padded = -(-rows // LANES) * LANES
    layers, chans, reach = w_value.shape[0], w_value.shape[2], taps.shape[1]
    part, step = depth // tp, min(2 * LANES, chans)
    slots = 2 * (chans // step)
    pad = -(-(reach - 1) // 16) * 16
    share = w_out.shape[1] // grp
    cuts = CUTS
    vmem, dma = pltpu.VMEM, pltpu.SemaphoreType.DMA
    there = pl.BlockSpec(memory_space=pltpu.HBM)
    return pl.pallas_call(
        functools.partial(gated_conv, layers, sp, tp),
        out_shape=jax.ShapeDtypeStruct((rows, depth), BF16),
        in_specs=[there] * 8,
        out_specs=pl.BlockSpec(memory_space=pltpu.VMEM),
        scratch_shapes=[
            vmem((rows, depth), BF16),
            vmem((layers, depth), F32),
            vmem((reach, layers, chans), F32),
            vmem((layers, chans), F32),
            vmem((layers, chans), F32),
            vmem((layers, rows, depth), BF16),
            vmem((layers, 2, depth, chans), BF16),
            vmem((layers, sp, grp, share, depth), BF16),
            vmem((max(layers - 1, 1), 2, depth, chans // step // 2 * step), BF16),
            vmem((layers, tp, rows, part), BF16),
            vmem((layers, tp, rows, part), BF16),
            vmem((layers, tp, sp + 1, rows, part), BF16),
            vmem((layers, 2, sp, slots, rows, step), BF16),
            vmem((layers, 2, sp, slots, rows, step), BF16),
            vmem((2, rows, step), F32),
            vmem((layers, tp, 8, padded), F32),
            vmem((rows, LANES), F32),
            vmem((layers, tp, 8, padded), F32),
            vmem((layers, chans // step, pad, step), BF16),
            vmem((layers, chans // step, pad, step), BF16),
            vmem((pad + rows, chans), F32),
            vmem((rows, chans), F32),
            vmem((layers, tp, rows, chans), BF16),
            dma((5,)), dma((layers, 2)),
            dma((layers, tp)), dma((layers, tp)), dma((layers, sp)),
            dma((layers, tp, sp + 1)), dma((layers, tp, sp + 1)), dma((layers, tp, sp + 1)),
            dma((layers, 2, sp, slots)), dma((layers, 2, sp, slots)),
            dma((layers, tp)), dma((layers, tp)), dma((layers, tp)), dma((layers, tp)),
            dma((layers, chans // step)), dma((layers, chans // step)),
            dma((layers, tp)), dma((layers, tp)), dma((layers, tp)),
            dma((layers, grp)), dma((layers, 2, sp, cuts)), dma((layers, sp, cuts)),
            dma((layers, grp, sp, cuts)), dma((layers, sp, grp, cuts)),
            dma((layers, 2, LOTS)), dma((layers, 2, LOTS)),
            dma((layers, grp, 2, LOTS)), dma((layers, 2, grp, LOTS)),
        ],
        compiler_params=pltpu.CompilerParams(
            collective_id=0, has_side_effects=True, vmem_limit_bytes=60 * 2**20
        ),
    )(
        tokens, rms_gain, w_value, w_gate, jnp.transpose(taps, (1, 0, 2)), ln_gain, ln_bias, w_out
    )


def fits(tokens, w_value, taps, w_out):
    sp, tp, grp = (lax.axis_size(a) for a in ("sp", "tp", "grp"))
    rows, depth = tokens.shape
    chans = w_value.shape[2]
    return (
        sp == tp
        and tp % 2 == 0
        and depth % (tp * LANES) == 0
        and chans % (LANES * grp) == 0
        and w_out.shape[1] % (16 * grp * CUTS) == 0
        and w_out.shape[1] == chans
        and depth % (16 * grp * LOTS) == 0
        and chans % min(2 * LANES, chans) == 0
        and rows % 16 == 0
        and rows >= -(-(taps.shape[1] - 1) // 16) * 16
    )


def shards(tokens, rms_gain, w_value, w_gate, taps, ln_gain, ln_bias, w_out):
    if fits(tokens, w_value, taps, w_out):
        return fused(tokens, rms_gain, w_value, w_gate, taps, ln_gain, ln_bias, w_out)
    layers = w_value.shape[0]
    tok_rows = tokens.shape[0]
    chans = w_value.shape[2]
    all_chans = chans * lax.axis_size("tp")
    reach = taps.shape[1]
    current = tokens
    for layer in range(layers):
        whole_rows = lax.all_gather(current, "tp", axis=1, tiled=True)
        normed = to_depth(norm_rows(whole_rows.astype(jnp.float32), rms_gain[layer]))
        both = jnp.concatenate([w_value[layer], w_gate[layer]], axis=1)
        both = summed(jnp.dot(normed, both, preferred_element_type=jnp.float32))
        glu = (both[:, :chans] * jax.nn.sigmoid(both[:, chans:])).astype(jnp.bfloat16)
        earlier = passed_along(glu[tok_rows - (reach - 1) :], "sp", 1)
        extended = jnp.concatenate([earlier, glu], axis=0).astype(jnp.float32)
        conv = jnp.zeros((tok_rows, chans), jnp.float32)
        for k in range(reach):
            conv = conv + taps[layer, k][None, :] * extended[k : k + tok_rows]
        total, total_sq = lax.psum((jnp.sum(conv, axis=1), jnp.sum(conv * conv, axis=1)), "tp")
        mean = total / all_chans
        var = total_sq / all_chans - mean * mean
        shaped = (conv - mean[:, None]) * lax.rsqrt(var + 1e-05)[:, None] * ln_gain[layer][
            None, :
        ] + ln_bias[layer][None, :]
        act = jax.nn.silu(shaped).astype(jnp.bfloat16)
        act_all = to_depth(lax.all_gather(act, "tp", axis=1, tiled=True))
        branch = summed(jnp.dot(act_all, w_out[layer], preferred_element_type=jnp.float32))
        current = (current.astype(jnp.float32) + branch).astype(jnp.bfloat16)
    return current


def solution(mesh):
    return jax.shard_map(
        shards,
        mesh=mesh,
        in_specs=(
            P(("grp", "sp"), "tp"),
            P(),
            P(None, "sp", "tp"),
            P(None, "sp", "tp"),
            P(None, None, "tp"),
            P(None, "tp"),
            P(None, "tp"),
            P(None, "sp", "tp"),
        ),
        out_specs=P(("grp", "sp"), "tp"),
        check_vma=False,
    )
```

```python
import functools

import jax
import jax.numpy as jnp
from jax import lax
from jax.experimental import pallas as pl
from jax.experimental.pallas import tpu as pltpu
from jax.sharding import PartitionSpec as P

LANES = 128
BF16, F32 = jnp.bfloat16, jnp.float32
LOTS = 2
CUTS = 8

FIRST = {
    (1, 0): ("start", "start", "gathered", "gathered"),
    (2, 0): ("start", "start", "scattered", "turned"),
    (3, 0): ("start", "start", "scattered", "finished"),
    (0, 1): ("gathered", "gathered", "summed", "summed"),
    (1, 1): ("gathered", "gathered", "summed", "summed"),
    (2, 1): ("gathered summed", "gathered finished", "gathered finished", "counted"),
    (0, 2): ("summed", "summed", "counted", "counted"),
    (1, 2): ("counted", "counted", "closed", "closed"),
}
LATER = {
    (1, 0): ("start", "start", "start", "start"),
    (2, 0): ("tail", "tail", "tail", "tail"),
    (3, 0): ("tail", "tail", "tail", "tail"),
    (0, 1): ("gathered", "gathered", "gathered", "gathered"),
    (1, 1): ("before", "before", "gathered", "gathered"),
    (2, 1): ("start", "before", "scattered", "finished"),
    (0, 2): ("summed", "summed", "summed", "summed"),
    (1, 2): ("summed", "summed", "counted", "counted"),
    (0, 3): ("counted", "counted", "closed", "closed"),
}


def passed_along(block, axis, distance):
    devices = range(lax.axis_size(axis))
    route = [(i - distance, i) for i in devices if i - distance in devices]
    return lax.ppermute(block, axis, route)


def norm_rows(wide, gain):
    return (wide * lax.rsqrt(jnp.mean(wide * wide, axis=1, keepdims=True) + 1e-06) * gain).astype(
        jnp.bfloat16
    )


def to_depth(rows):
    return lax.all_to_all(rows, "sp", split_axis=1, concat_axis=0, tiled=True)


def summed(partial):
    sp = lax.axis_size("sp")
    rows = partial.shape[0] // sp
    parts = partial.astype(jnp.bfloat16).reshape(sp, rows, partial.shape[1])
    parts = lax.all_to_all(parts, "sp", split_axis=0, concat_axis=0, tiled=True)
    return jnp.sum(parts.astype(jnp.float32), axis=0)


def send(src, dst, send_sem, recv_sem, **where):
    return pltpu.make_async_remote_copy(
        src_ref=src,
        dst_ref=dst,
        send_sem=send_sem,
        recv_sem=recv_sem,
        device_id=where,
        device_id_type=pl.DeviceIdType.MESH,
    )


def gated_conv(
    layers, sp, tp,
    h_hbm, gain_hbm, wv_hbm, wg_hbm, taps_hbm, lng_hbm, lnb_hbm, wo_hbm, out_ref,
    h_ref, gain_ref, taps_ref, lng_ref, lnb_ref, mid,
    wvg, wo, lent, pieces, spread, xs, going, coming, own, sq, sq_sum, stat,
    halo_out, halo_in, ext, conv, acts,
    i_sem, w_sem, a_send, a_recv, b_send, c_send, c_relay, x_recv, r_send, r_recv,
    q_send, q_recv, s_send, s_recv, h_send, h_recv, g_send, g_recv,
    o_sem, z_send, z_recv, y_send, y_recv, v_send, v_recv, u_send, u_recv,
):
    s, c, g = lax.axis_index("sp"), lax.axis_index("tp"), lax.axis_index("grp")
    grp, share = wo.shape[2], wo.shape[3]
    padded = sq.shape[3]
    rows, depth = h_ref.shape
    chans = taps_ref.shape[2]
    part = depth // tp
    step = going.shape[-1]
    chunks = chans // step
    pairs = tp // 2
    sibling = c + 1 - 2 * (c % 2)
    reach = taps_ref.shape[0]
    pad = halo_in.shape[2]
    cuts = z_recv.shape[2]
    early = cuts // 2
    cut = share // cuts
    bands = stat.shape[1]
    band = rows // bands
    lots = v_recv.shape[2]
    lot = depth // (grp * lots)
    early_lots = 2 * lots
    kept = chunks - lent.shape[3] // step
    at_end = (s == 0) | (s == sp - 1)
    at_host = (s == 1) | (s == sp - 2)
    partner = (s == 0) + (sp - 2) * (s == sp - 1) + (sp - 1) * (s == sp - 2)

    first_loads = [
        pltpu.make_async_copy(h_hbm, h_ref, i_sem.at[0]),
        pltpu.make_async_copy(
            gain_hbm.at[:, pl.ds(pl.multiple_of(c * depth, LANES), depth)], gain_ref, i_sem.at[1]
        ),
    ]
    small_loads = [
        pltpu.make_async_copy(taps_hbm, taps_ref, i_sem.at[2]),
        pltpu.make_async_copy(lng_hbm, lng_ref, i_sem.at[3]),
        pltpu.make_async_copy(lnb_hbm, lnb_ref, i_sem.at[4]),
    ]
    in_loads = [
        (
            pltpu.make_async_copy(wv_hbm.at[l], wvg.at[l, 0], w_sem.at[l, 0]),
            pltpu.make_async_copy(wg_hbm.at[l], wvg.at[l, 1], w_sem.at[l, 1]),
        )
        for l in range(layers)
    ]
    out_loads = [
        [
            pltpu.make_async_copy(
                wo_hbm.at[l, pl.ds(n * share, share)], wo.at[l, s, n], o_sem.at[l, n]
            )
            for n in range(grp)
        ]
        for l in range(layers)
    ]
    for load in first_loads:
        load.start()
    for l in range(layers):
        for load in out_loads[l]:
            load.start()
        for load in in_loads[l]:
            load.start()
    for load in small_loads:
        load.start()

    barrier = pltpu.get_barrier_semaphore()
    for j in range(1, tp):
        pl.semaphore_signal(
            barrier, inc=1, device_id={"tp": (c + j) % tp}, device_id_type=pl.DeviceIdType.MESH
        )
    for j in range(1, sp):
        pl.semaphore_signal(
            barrier, inc=1, device_id={"sp": (s + j) % sp}, device_id_type=pl.DeviceIdType.MESH
        )
    for j in range(1, grp):
        pl.semaphore_signal(
            barrier, inc=1, device_id={"grp": (g + j) % grp}, device_id_type=pl.DeviceIdType.MESH
        )

    def to_row(column):
        blank = -column.shape[0] % LANES
        column = jnp.concatenate([column, jnp.zeros((blank, LANES), F32)], axis=0)
        return jnp.sum(column.T, axis=0, keepdims=True)

    def to_column(row, size):
        return jnp.broadcast_to(row, (LANES, row.shape[1])).T[:size, 0:1]

    def all_of(block, sem):
        return send(block, block, sem, sem, tp=sibling)

    def turn(i):
        return ((c // 2 + 1 + i // 2) % pairs) * 2 + (c + 1 + i) % 2

    def a_copy(l, to, frm):
        return send(
            pieces.at[l, to], spread.at[l, frm], a_send.at[l], a_recv.at[l, frm], tp=to
        )

    def q_copy(l, to, frm):
        return send(sq.at[l, frm], sq.at[l, frm], q_send.at[l], q_recv.at[l], tp=to)

    def prepare(l, p, block):
        wide = block.astype(F32)
        total = sq_sum[...]
        for lane in range(0, part, LANES):
            tile = wide[:, lane : lane + LANES]
            total = total + tile * tile
        sq_sum[...] = total
        gain = gain_ref[l : l + 1, pl.ds(pl.multiple_of(p * part, LANES), part)]
        pieces[l, p] = (wide * gain).astype(BF16)

    def hand_out(l, p):
        @pl.when(p != c)
        def _():
            a_copy(l, p, c).start()

        @pl.when(p == c)
        def _():
            spread[l, c] = pieces[l, c]

    def hand_out_squares(l):
        sq[l, c] = jnp.broadcast_to(to_row(sq_sum[...]), sq.shape[2:])
        for j in range(1, tp):
            q_copy(l, (c + j) % tp, c).start()

    def beyond(left):
        return (1 - left) * (sp - 1 - s) + left * s

    def z_copy(l, left, o, k):
        rows_k = pl.ds(k * cut, cut)
        return send(
            wo.at[l, o, g, rows_k],
            wo.at[l, o, g, rows_k],
            z_send.at[l, left],
            z_recv.at[l, o, k],
            sp=s + 1 - 2 * left,
        )

    def y_copy(l, j, o, n, k):
        rows_k = pl.ds(k * cut, cut)
        return send(
            wo.at[l, o, n, rows_k],
            wo.at[l, o, n, rows_k],
            y_send.at[l, j],
            y_recv.at[l, n],
            grp=(g + j) % grp,
        )

    def z_take(l, o, k):
        rows_k = pl.ds(k * cut, cut)
        send(
            wo.at[l, o, g, rows_k],
            wo.at[l, o, g, rows_k],
            z_send.at[l, 0],
            z_recv.at[l, o, k],
            sp=(s + 1) % sp,
        ).wait_recv()
        for j in range(1, grp):
            y_copy(l, j, o, g, k).start()

    def moment(l, ahead, i, k):
        if l == 0:
            table = FIRST
        else:
            table = LATER
        points = table.get((ahead, i), ("closed",) * 4)[4 * k // cuts]
        return points.split() if " " in points else (points, points)

    def fill(l, point):
        for left in range(2):
            for ahead in range(sp):
                steps = []
                for i in range(sp - ahead):
                    for k in range(cuts):
                        taken, sent_on = moment(l, min(ahead, 3), i, k)
                        if i > 0 and taken == point:
                            steps.append((i, k, True))
                        if ahead > 0 and sent_on == point:
                            steps.append((i, k, False))

                if steps:

                    @pl.when(beyond(left) == ahead)
                    def _():
                        for i, k, take in steps:
                            o = s + (2 * left - 1) * i
                            if take:
                                z_take(l, o, k)
                            else:
                                z_copy(l, left, o, k).start()

    def lends(l):
        return l > 0 and sp >= 4 and kept < chunks

    def sent_chunks(l, d):
        if not lends(l):
            return chunks
        return chunks - (chunks - kept) * (at_end & (d == partner)).astype(jnp.int32)

    def v_copy(l, t):
        half, q = t % 2, t // 2
        rows_q = pl.ds(pl.multiple_of((g * lots + q) * lot, lot), lot)
        return send(
            wvg.at[l, half, rows_q, pl.ds(kept * step, (chunks - kept) * step)],
            lent.at[l - 1, half, rows_q],
            v_send.at[l - 1],
            v_recv.at[l - 1, half, q],
            sp=partner,
        )

    def u_copy(l, j, t, n):
        half, q = t % 2, t // 2
        rows_q = pl.ds(pl.multiple_of((n * lots + q) * lot, lot), lot)
        return send(
            lent.at[l - 1, half, rows_q],
            lent.at[l - 1, half, rows_q],
            u_send.at[l - 1, j],
            u_recv.at[l - 1, n],
            grp=(g + j) % grp,
        )

    def lot_of(l):
        return lent.at[l - 1, pl.ds(0, 2), pl.ds(0, depth // grp)]

    def lend_out(l, first, last):
        if lends(l):

            @pl.when(at_end)
            def _():
                for t in range(first, last):
                    v_copy(l, t).start()

    def lend_in(l, first, last):
        if lends(l):

            @pl.when(at_host)
            def _():
                for t in range(first, last):
                    v_copy(l, t).wait_recv()
                    for j in range(1, grp):
                        u_copy(l, j, t, g).start()

    def place(j):
        left = (j + 2 * s // sp) % 2
        k = j // 2
        d = (1 - left) * (sp - 1 - k) + left * k
        return left, d, (1 - 2 * left) * (d - s) > 0

    def each(body):
        def one(j, carry):
            left, d, valid = place(j)

            @pl.when(valid)
            def _():
                body(j, left, d)

            return carry

        lax.fori_loop(0, 2 * (sp - 1), one, 0)

    def behind(left):
        return (1 - left) * s + left * (sp - 1 - s)

    def upstream(left):
        return behind(left) > 0

    def b_copy(l, to, frm):
        return send(
            spread.at[l, to], xs.at[l, c, frm], b_send.at[l], x_recv.at[l, c, frm], sp=to
        )

    def c_copy(l, to, d, sem):
        return send(xs.at[l, c, d], xs.at[l, c, d], sem, x_recv.at[l, c, d], tp=to)

    def relay(l, p, d):
        return send(
            xs.at[l, p, d], xs.at[l, p, d], c_relay.at[l, p], x_recv.at[l, p, d], tp=sibling
        )

    def r_copy(l, left, d, slot):
        return send(
            going.at[l, left, d, slot],
            coming.at[l, left, d, slot],
            r_send.at[l, left, slot],
            r_recv.at[l, left, d, slot],
            sp=s + 1 - 2 * left,
        )

    def h_copy(l, to, i):
        return send(
            halo_out.at[l, i], halo_in.at[l, i], h_send.at[l, i], h_recv.at[l, i], sp=to
        )

    def s_copy(l, b, to, frm):
        return send(
            stat.at[l, b, frm], stat.at[l, b, frm], s_send.at[l, b], s_recv.at[l, b], tp=to
        )

    def g_copy(l, b, to, p):
        block = acts.at[l, p, pl.ds(b * band, band)]
        return send(block, block, g_send.at[l, b], g_recv.at[l, p, b], tp=to)

    def layer_of(l):
        slots = 2 * chunks
        inner = sp == 4 and slots >= 2
        mids = 1 - at_end.astype(jnp.int32)

        def held(e):
            @pl.when(e != c)
            def _():
                a_copy(l, c, e).wait_recv()

        def scatter(j, left, d):
            held(d)
            b_copy(l, d, s).start()

        if l > 0:
            fill(l, "before")
            lend_in(l, 0, lots)
        each(scatter)
        fill(l, "scattered")
        held(s)
        xs[l, c, s] = spread[l, s]
        if lends(l):

            @pl.when(at_host)
            def _():
                xs[l, c, sp] = spread[l, partner]

        def gather(d, arriving=True):
            if arriving:
                relay(l, c, d).wait_recv()
            for j in range(1, pairs):
                c_copy(l, (c + 2 * j) % tp, d, c_send.at[l, j]).start()
            c_copy(l, sibling, d, c_send.at[l, 0]).start()

        gather(s, False)
        if inner:
            gather(place(0)[1])
            gather(place(1 + at_end.astype(jnp.int32))[1])
        else:
            each(lambda j, left, d: gather(d))
        if l == 0:
            for load in in_loads[l]:
                load.wait()

        def ready(d):
            for j in range(1, pairs):
                p = (c + 2 * j) % tp
                relay(l, p, d).wait_recv()
                relay(l, p, d).start()
            for j in range(pairs):
                relay(l, (sibling + 2 * j) % tp, d).wait_recv()

        def product(d, weight, at):
            acc = jnp.zeros((rows, step), F32)
            for p in range(tp):
                acc = acc + jnp.dot(
                    xs[l, p, d],
                    weight[p * part : (p + 1) * part, pl.ds(at, step)],
                    preferred_element_type=F32,
                )
            return acc

        def r_arrived(left, d, slot):
            send(
                going.at[l, left, d, slot],
                coming.at[l, left, d, slot],
                r_send.at[l, left, slot],
                r_recv.at[l, left, d, slot],
                sp=(s + 1) % sp,
            ).wait_recv()

        def partial(slot, left, d):
            half, i = slot % 2, slot // 2

            @pl.when(slot == 0)
            def _():
                ready(d)

            own[half] = product(d, wvg.at[l, half], pl.multiple_of(i * step, step))

            @pl.when(upstream(left))
            def _():
                r_arrived(left, d, slot)
                own[half] += coming[l, left, d, slot].astype(F32)

            going[l, left, d, slot] = own[half].astype(BF16)
            r_copy(l, left, d, slot).start()

        def turn_slot(t):
            if not inner:
                return t // slots, t % slots
            u = t - 2
            woven = ((u >= 0) & (u < 2 * slots)).astype(jnp.int32)
            aside = woven * (1 - u % 2) * mids
            k = jnp.where(woven == 1, 2 + u // 2, jnp.where(u < 0, t, t - slots))
            k = mids * k + (1 - mids) * t
            j = aside + (1 - aside) * 2 * (k // slots)
            return j, aside * (u // 2) + (1 - aside) * (k % slots)

        def advance(t, carry):
            j, slot = turn_slot(t)
            left, d, valid = place(j)

            @pl.when(valid & (slot < 2 * sent_chunks(l, d)))
            def _():
                partial(slot, left, d)

            @pl.when(t == 0)
            def _():
                if inner:
                    gather(place(2 + 2 * at_end.astype(jnp.int32))[1])
                if lends(l):

                    @pl.when(at_host)
                    def _():
                        gather(sp, False)

                lend_in(l, lots, early_lots)
                fill(l, "gathered")
                lend_out(l, early_lots, 2 * lots)

            @pl.when(t == slots - 1 + (mids * (slots - 2) if inner else 0))
            def _():
                fill(l, "turned")
                lend_in(l, early_lots, 2 * lots)

            @pl.when(t == 2 * slots - 1)
            def _():
                fill(l, "halfway")

            return carry

        lax.fori_loop(0, slots * (3 if inner else 2 * (sp - 1)), advance, 0)
        fill(l, "summed")
        ready(s)
        if lends(l):

            @pl.when(at_host)
            def _():
                ready(sp)
                for j in range(1, grp):
                    all_of(lot_of(l), u_recv.at[l - 1, (g + j) % grp]).wait_recv()

        all_of(sq.at[l, pl.ds(0, tp - 1)], q_recv.at[l]).wait_recv()
        squares = sq[l, 0]
        for p in range(1, tp):
            squares = squares + sq[l, p]
        scale = to_column(lax.rsqrt(squares[0:1] / (depth * tp) + 1e-06), rows)

        def finish(i, carry):
            at = pl.multiple_of(i * step, step)
            for half in range(2):
                slot = 2 * i + half
                own[half] = product(s, wvg.at[l, half], at)
                if lends(l):

                    @pl.when(at_host & (i >= kept))
                    def _():
                        own[half] += product(
                            sp, lent.at[l - 1, half], pl.multiple_of(at - kept * step, step)
                        )

                for left in range(2):
                    expected = upstream(left)
                    if lends(l):
                        expected = expected & jnp.logical_not(
                            at_host & (behind(left) == 1) & (i >= kept)
                        )

                    @pl.when(expected)
                    def _():
                        r_arrived(left, s, slot)
                        own[half] += coming[l, left, s, slot].astype(F32)

            glu = (own[0] * scale * jax.nn.sigmoid(own[1] * scale)).astype(BF16)
            ext[pad:, pl.ds(at, step)] = glu.astype(F32)
            halo_out[l, i] = glu[rows - pad :]

            @pl.when(s < sp - 1)
            def _():
                h_copy(l, s + 1, i).start()

            return carry

        lax.fori_loop(0, chunks, finish, 0)
        if l == 0:
            for load in small_loads:
                load.wait()
        fill(l, "finished")
        first = pad - (reach - 1)

        def halo_in_place(i, carry):
            lanes = pl.ds(pl.multiple_of(i * step, step), step)

            @pl.when(s > 0)
            def _():
                h_copy(l, (s + 1) % sp, i).wait_recv()
                ext[:pad, lanes] = halo_in[l, i].astype(F32)

            @pl.when(s == 0)
            def _():
                ext[:pad, lanes] = jnp.zeros((pad, step), F32)

            return carry

        def strip(b, i, carry):
            lanes = pl.ds(pl.multiple_of(i * LANES, LANES), LANES)
            above = first + b * band
            acc = jnp.zeros((band, LANES), F32)
            for k in range(reach):
                acc = acc + taps_ref[k, l : l + 1, lanes] * ext[above + k : above + k + band, lanes]
            conv[b * band : (b + 1) * band, lanes] = acc
            return carry

        half = stat.shape[3] // 2
        for b in reversed(range(bands)):
            if b == 0:
                lax.fori_loop(0, chunks, halo_in_place, 0)
            lax.fori_loop(0, chans // LANES, functools.partial(strip, b), 0)
            total = jnp.zeros((band, LANES), F32)
            total_sq = jnp.zeros((band, LANES), F32)
            for at in range(0, chans, LANES):
                tile = conv[b * band : (b + 1) * band, at : at + LANES]
                total = total + tile
                total_sq = total_sq + tile * tile
            stat[l, b, c] = jnp.concatenate(
                [
                    jnp.broadcast_to(to_row(t), (half, stat.shape[4]))
                    for t in (total, total_sq)
                ],
                axis=0,
            )
            for j in range(1, tp):
                s_copy(l, b, (c + j) % tp, c).start()
        fill(l, "counted")
        if l + 1 < layers:
            for load in out_loads[l + 1]:
                load.wait()
            for load in in_loads[l + 1]:
                load.wait()
            fill(l + 1, "tail")
            lend_out(l + 1, 0, early_lots)
        for b in reversed(range(bands)):
            all_of(stat.at[l, b, pl.ds(0, tp - 1)], s_recv.at[l, b]).wait_recv()
            stats = stat[l, b, 0]
            for p in range(1, tp):
                stats = stats + stat[l, b, p]
            mean = stats[0:1] / (chans * tp)
            var = stats[half : half + 1] / (chans * tp) - mean * mean
            inv = to_column(lax.rsqrt(var + 1e-05), band)
            mean = to_column(mean, band)
            here = slice(b * band, (b + 1) * band)
            for at in range(0, chans, LANES):
                lanes = slice(at, at + LANES)
                shaped = (conv[here, lanes] - mean) * inv * lng_ref[l : l + 1, lanes] + lnb_ref[
                    l : l + 1, lanes
                ]
                acts[l, c, here, lanes] = (shaped / (1.0 + jnp.exp(-shaped))).astype(BF16)
            for j in range(1, pairs):
                g_copy(l, b, (c + 2 * j) % tp, c).start()
            g_copy(l, b, sibling, c).start()
        fill(l, "closed")
        if l + 1 < layers:
            fill(l + 1, "start")
        for b in reversed(range(bands)):
            for j in range(1, pairs):
                p = (c + 2 * j) % tp
                g_copy(l, b, sibling, p).wait_recv()
                g_copy(l, b, sibling, p).start()
        for j in range(pairs):
            p = (sibling + 2 * j) % tp
            for b in range(bands):
                g_copy(l, b, sibling, p).wait_recv()
        for j in range(1, grp):
            all_of(wo.at[l, pl.ds(0, sp - 1), 0], y_recv.at[l, (g + j) % grp]).wait_recv()

        sq_sum[...] = jnp.zeros_like(sq_sum)

        def project(i, carry):
            p = turn(i)
            lanes = pl.ds(pl.multiple_of(p * part, LANES), part)
            acc = jnp.zeros((rows, part), F32)
            for e in range(tp):
                for n in range(grp):
                    acc = acc + jnp.dot(
                        acts[l, e, :, n * share : (n + 1) * share],
                        wo[l, e, n, :, lanes],
                        preferred_element_type=F32,
                    )
            before = h_ref if l == 0 else mid.at[l - 1]
            block = (before[:, lanes].astype(F32) + acc).astype(BF16)
            if l + 1 < layers:
                mid[l, :, lanes] = block
                prepare(l + 1, p, block)
                hand_out(l + 1, p)
            else:
                out_ref[:, lanes] = block
            return carry

        lax.fori_loop(0, tp, project, 0)
        if l + 1 < layers:
            hand_out_squares(l + 1)

    sq_sum[...] = jnp.zeros_like(sq_sum)
    for load in first_loads:
        load.wait()
    for p in range(tp):
        prepare(0, p, h_ref[:, p * part : (p + 1) * part])
    for load in out_loads[0]:
        load.wait()
    pl.semaphore_wait(barrier, tp + sp + grp - 3)

    def first_hand_out(i, carry):
        hand_out(0, turn(i))
        return carry

    lax.fori_loop(0, tp, first_hand_out, 0)
    fill(0, "start")
    hand_out_squares(0)
    for l in range(layers):
        layer_of(l)

    def sent(block, sem):
        all_of(block, sem).wait_send()

    def sent_some(count, most, block, sem):
        for n in range(1, most + 1):

            @pl.when(count == n)
            def _():
                sent(block(n), sem)

    for l in range(layers):
        sent(pieces.at[l, pl.ds(0, tp - 1)], a_send.at[l])
        sent(sq.at[l, pl.ds(0, tp - 1)], q_send.at[l])
        sent(spread.at[l, pl.ds(0, sp - 1)], b_send.at[l])
        for b in range(bands):
            sent(stat.at[l, b, pl.ds(0, tp - 1)], s_send.at[l, b])
            sent(acts.at[l, pl.ds(0, tp - 1), pl.ds(b * band, band)], g_send.at[l, b])

        def exchanged(n):
            for j in range(pairs):
                sent(xs.at[l, 0, pl.ds(0, n)], c_send.at[l, j])
            for j in range(1, pairs):
                sent(xs.at[l, 0, pl.ds(0, n)], c_relay.at[l, (c + 2 * j) % tp])

        if lends(l):
            for host in (False, True):

                @pl.when(at_host == host)
                def _():
                    exchanged(sp + host)

            @pl.when(at_host)
            def _():
                for j in range(1, grp):
                    sent(lot_of(l), u_send.at[l - 1, j])

            @pl.when(at_end)
            def _():
                sent(lot_of(l), v_send.at[l - 1])
        else:
            exchanged(sp)

        for left in range(2):
            for slot in range(2 * chunks):
                skipped = at_end.astype(jnp.int32) * int(lends(l) and slot >= 2 * kept)
                sent_some(
                    beyond(left) - skipped,
                    sp - 1,
                    lambda n: going.at[l, left, pl.ds(0, n), slot],
                    r_send.at[l, left, slot],
                )
            sent_some(
                (behind(left) + 1) * (beyond(left) > 0).astype(jnp.int32),
                sp - 1,
                lambda n: wo.at[l, pl.ds(0, n), 0],
                z_send.at[l, left],
            )
        for j in range(1, grp):
            sent(wo.at[l, pl.ds(0, sp - 1), 0], y_send.at[l, j])

        @pl.when(s < sp - 1)
        def _():
            for i in range(chunks):
                h_copy(l, s + 1, i).wait_send()


def fused(tokens, rms_gain, w_value, w_gate, taps, ln_gain, ln_bias, w_out):
    sp, tp, grp = (lax.axis_size(a) for a in ("sp", "tp", "grp"))
    rows, depth = tokens.shape
    padded = -(-rows // LANES) * LANES
    layers, chans, reach = w_value.shape[0], w_value.shape[2], taps.shape[1]
    part, step = depth // tp, min(2 * LANES, chans)
    slots = 2 * (chans // step)
    pad = -(-(reach - 1) // 16) * 16
    share = w_out.shape[1] // grp
    cuts = CUTS
    bands = 2 if rows % 32 == 0 and rows // 2 >= pad else 1
    vmem, dma = pltpu.VMEM, pltpu.SemaphoreType.DMA
    there = pl.BlockSpec(memory_space=pltpu.HBM)
    return pl.pallas_call(
        functools.partial(gated_conv, layers, sp, tp),
        out_shape=jax.ShapeDtypeStruct((rows, depth), BF16),
        in_specs=[there] * 8,
        out_specs=pl.BlockSpec(memory_space=pltpu.VMEM),
        scratch_shapes=[
            vmem((rows, depth), BF16),
            vmem((layers, depth), F32),
            vmem((reach, layers, chans), F32),
            vmem((layers, chans), F32),
            vmem((layers, chans), F32),
            vmem((layers, rows, depth), BF16),
            vmem((layers, 2, depth, chans), BF16),
            vmem((layers, sp, grp, share, depth), BF16),
            vmem((max(layers - 1, 1), 2, depth, chans // step // 2 * step), BF16),
            vmem((layers, tp, rows, part), BF16),
            vmem((layers, tp, rows, part), BF16),
            vmem((layers, tp, sp + 1, rows, part), BF16),
            vmem((layers, 2, sp, slots, rows, step), BF16),
            vmem((layers, 2, sp, slots, rows, step), BF16),
            vmem((2, rows, step), F32),
            vmem((layers, tp, 8, padded), F32),
            vmem((rows, LANES), F32),
            vmem((layers, bands, tp, 8, -(-rows // bands // LANES) * LANES), F32),
            vmem((layers, chans // step, pad, step), BF16),
            vmem((layers, chans // step, pad, step), BF16),
            vmem((pad + rows, chans), F32),
            vmem((rows, chans), F32),
            vmem((layers, tp, rows, chans), BF16),
            dma((5,)), dma((layers, 2)),
            dma((layers,)), dma((layers, tp)), dma((layers,)),
            dma((layers, tp // 2)), dma((layers, tp)), dma((layers, tp, sp + 1)),
            dma((layers, 2, slots)), dma((layers, 2, sp, slots)),
            dma((layers,)), dma((layers,)), dma((layers, bands)), dma((layers, bands)),
            dma((layers, chans // step)), dma((layers, chans // step)),
            dma((layers, bands)), dma((layers, tp, bands)),
            dma((layers, grp)), dma((layers, 2)), dma((layers, sp, cuts)),
            dma((layers, grp)), dma((layers, grp)),
            dma((layers,)), dma((layers, 2, LOTS)), dma((layers, grp)), dma((layers, grp)),
        ],
        compiler_params=pltpu.CompilerParams(
            collective_id=0, has_side_effects=True, vmem_limit_bytes=60 * 2**20
        ),
    )(
        tokens, rms_gain, w_value, w_gate, jnp.transpose(taps, (1, 0, 2)), ln_gain, ln_bias, w_out
    )


def fits(tokens, w_value, taps, w_out):
    sp, tp, grp = (lax.axis_size(a) for a in ("sp", "tp", "grp"))
    rows, depth = tokens.shape
    chans = w_value.shape[2]
    return (
        sp == tp
        and tp % 2 == 0
        and depth % (tp * LANES) == 0
        and chans % (LANES * grp) == 0
        and w_out.shape[1] % (16 * grp * CUTS) == 0
        and w_out.shape[1] == chans
        and depth % (16 * grp * LOTS) == 0
        and chans % min(2 * LANES, chans) == 0
        and rows % 16 == 0
        and rows >= -(-(taps.shape[1] - 1) // 16) * 16
    )


def shards(tokens, rms_gain, w_value, w_gate, taps, ln_gain, ln_bias, w_out):
    if fits(tokens, w_value, taps, w_out):
        return fused(tokens, rms_gain, w_value, w_gate, taps, ln_gain, ln_bias, w_out)
    layers = w_value.shape[0]
    tok_rows = tokens.shape[0]
    chans = w_value.shape[2]
    all_chans = chans * lax.axis_size("tp")
    reach = taps.shape[1]
    current = tokens
    for layer in range(layers):
        whole_rows = lax.all_gather(current, "tp", axis=1, tiled=True)
        normed = to_depth(norm_rows(whole_rows.astype(jnp.float32), rms_gain[layer]))
        both = jnp.concatenate([w_value[layer], w_gate[layer]], axis=1)
        both = summed(jnp.dot(normed, both, preferred_element_type=jnp.float32))
        glu = (both[:, :chans] * jax.nn.sigmoid(both[:, chans:])).astype(jnp.bfloat16)
        earlier = passed_along(glu[tok_rows - (reach - 1) :], "sp", 1)
        extended = jnp.concatenate([earlier, glu], axis=0).astype(jnp.float32)
        conv = jnp.zeros((tok_rows, chans), jnp.float32)
        for k in range(reach):
            conv = conv + taps[layer, k][None, :] * extended[k : k + tok_rows]
        total, total_sq = lax.psum((jnp.sum(conv, axis=1), jnp.sum(conv * conv, axis=1)), "tp")
        mean = total / all_chans
        var = total_sq / all_chans - mean * mean
        shaped = (conv - mean[:, None]) * lax.rsqrt(var + 1e-05)[:, None] * ln_gain[layer][
            None, :
        ] + ln_bias[layer][None, :]
        act = jax.nn.silu(shaped).astype(jnp.bfloat16)
        act_all = to_depth(lax.all_gather(act, "tp", axis=1, tiled=True))
        branch = summed(jnp.dot(act_all, w_out[layer], preferred_element_type=jnp.float32))
        current = (current.astype(jnp.float32) + branch).astype(jnp.bfloat16)
    return current


def solution(mesh):
    return jax.shard_map(
        shards,
        mesh=mesh,
        in_specs=(
            P(("grp", "sp"), "tp"),
            P(),
            P(None, "sp", "tp"),
            P(None, "sp", "tp"),
            P(None, None, "tp"),
            P(None, "tp"),
            P(None, "tp"),
            P(None, "sp", "tp"),
        ),
        out_specs=P(("grp", "sp"), "tp"),
        check_vma=False,
    )
```

```python
import functools

import jax
import jax.numpy as jnp
from jax import lax
from jax.experimental import pallas as pl
from jax.experimental.pallas import tpu as pltpu
from jax.sharding import PartitionSpec as P

LANES = 128
BF16, F32 = jnp.bfloat16, jnp.float32
LOTS = 2
CUTS = 8

FIRST = {
    (1, 0): ("start", "start", "gathered", "gathered"),
    (2, 0): ("start", "start", "scattered", "turned"),
    (3, 0): ("start", "start", "scattered", "finished"),
    (0, 1): ("gathered", "gathered", "summed", "summed"),
    (1, 1): ("gathered", "gathered", "turned summed", "summed"),
    (2, 1): ("gathered summed", "gathered finished", "gathered finished", "counted"),
    (0, 2): ("summed", "summed", "counted", "counted"),
    (1, 2): ("counted", "counted", "closed", "closed"),
}
LATER = {
    (1, 0): ("start", "start", "start", "start"),
    (2, 0): ("tail", "tail", "tail", "tail"),
    (3, 0): ("tail", "tail", "tail", "tail"),
    (0, 1): ("gathered", "gathered", "gathered", "gathered"),
    (1, 1): ("before", "before", "gathered", "gathered"),
    (2, 1): ("start", "before", "scattered", "scattered"),
    (0, 2): ("summed", "summed", "summed", "summed"),
    (1, 2, 0): ("summed", "summed", "finished", "finished"),
    (1, 2, 1): ("summed", "summed", "summed", "summed"),
    (0, 3, 0): ("counted", "counted", "closed", "closed"),
    (0, 3, 1): ("counted", "counted", "counted", "closed"),
}


def passed_along(block, axis, distance):
    devices = range(lax.axis_size(axis))
    route = [(i - distance, i) for i in devices if i - distance in devices]
    return lax.ppermute(block, axis, route)


def norm_rows(wide, gain):
    return (wide * lax.rsqrt(jnp.mean(wide * wide, axis=1, keepdims=True) + 1e-06) * gain).astype(
        jnp.bfloat16
    )


def to_depth(rows):
    return lax.all_to_all(rows, "sp", split_axis=1, concat_axis=0, tiled=True)


def summed(partial):
    sp = lax.axis_size("sp")
    rows = partial.shape[0] // sp
    parts = partial.astype(jnp.bfloat16).reshape(sp, rows, partial.shape[1])
    parts = lax.all_to_all(parts, "sp", split_axis=0, concat_axis=0, tiled=True)
    return jnp.sum(parts.astype(jnp.float32), axis=0)


def send(src, dst, send_sem, recv_sem, **where):
    return pltpu.make_async_remote_copy(
        src_ref=src,
        dst_ref=dst,
        send_sem=send_sem,
        recv_sem=recv_sem,
        device_id=where,
        device_id_type=pl.DeviceIdType.MESH,
    )


def gated_conv(
    layers, sp, tp,
    h_hbm, gain_hbm, wv_hbm, wg_hbm, taps_hbm, lng_hbm, lnb_hbm, wo_hbm, out_ref,
    h_ref, gain_ref, taps_ref, lng_ref, lnb_ref, mid,
    wvg, wo, lent, pieces, spread, xs, going, coming, own, sq, sq_sum, stat,
    halo_out, halo_in, ext, conv, acts,
    i_sem, w_sem, a_send, a_recv, b_send, c_send, c_relay, x_recv, r_send, r_recv,
    q_send, q_recv, s_send, s_recv, h_send, h_recv, g_send, g_recv,
    o_sem, z_send, z_recv, y_send, y_recv, v_send, v_recv, u_send, u_recv,
):
    s, c, g = lax.axis_index("sp"), lax.axis_index("tp"), lax.axis_index("grp")
    grp, share = wo.shape[2], wo.shape[3]
    padded = sq.shape[3]
    rows, depth = h_ref.shape
    chans = taps_ref.shape[2]
    part = depth // tp
    step = going.shape[-1]
    chunks = chans // step
    pairs = tp // 2
    sibling = c + 1 - 2 * (c % 2)
    reach = taps_ref.shape[0]
    pad = halo_in.shape[2]
    cuts = z_recv.shape[2]
    early = cuts // 2
    cut = share // cuts
    bands = stat.shape[1]
    band = rows // bands
    lots = v_recv.shape[2]
    lot = depth // (grp * lots)
    early_lots = 2 * lots
    kept = chunks - lent.shape[3] // step
    at_end = (s == 0) | (s == sp - 1)
    at_host = (s == 1) | (s == sp - 2)
    partner = (s == 0) + (sp - 2) * (s == sp - 1) + (sp - 1) * (s == sp - 2)

    first_loads = [
        pltpu.make_async_copy(h_hbm, h_ref, i_sem.at[0]),
        pltpu.make_async_copy(
            gain_hbm.at[:, pl.ds(pl.multiple_of(c * depth, LANES), depth)], gain_ref, i_sem.at[1]
        ),
    ]
    small_loads = [
        pltpu.make_async_copy(taps_hbm, taps_ref, i_sem.at[2]),
        pltpu.make_async_copy(lng_hbm, lng_ref, i_sem.at[3]),
        pltpu.make_async_copy(lnb_hbm, lnb_ref, i_sem.at[4]),
    ]
    in_loads = [
        (
            pltpu.make_async_copy(wv_hbm.at[l], wvg.at[l, 0], w_sem.at[l, 0]),
            pltpu.make_async_copy(wg_hbm.at[l], wvg.at[l, 1], w_sem.at[l, 1]),
        )
        for l in range(layers)
    ]
    out_loads = [
        [
            pltpu.make_async_copy(
                wo_hbm.at[l, pl.ds(n * share, share)], wo.at[l, s, n], o_sem.at[l, n]
            )
            for n in range(grp)
        ]
        for l in range(layers)
    ]
    for load in first_loads:
        load.start()
    for l in range(layers):
        for load in out_loads[l]:
            load.start()
        for load in in_loads[l]:
            load.start()
    for load in small_loads:
        load.start()

    barrier = pltpu.get_barrier_semaphore()
    for j in range(1, tp):
        pl.semaphore_signal(
            barrier, inc=1, device_id={"tp": (c + j) % tp}, device_id_type=pl.DeviceIdType.MESH
        )
    for j in range(1, sp):
        pl.semaphore_signal(
            barrier, inc=1, device_id={"sp": (s + j) % sp}, device_id_type=pl.DeviceIdType.MESH
        )
    for j in range(1, grp):
        pl.semaphore_signal(
            barrier, inc=1, device_id={"grp": (g + j) % grp}, device_id_type=pl.DeviceIdType.MESH
        )

    def to_row(column):
        blank = -column.shape[0] % LANES
        column = jnp.concatenate([column, jnp.zeros((blank, LANES), F32)], axis=0)
        return jnp.sum(column.T, axis=0, keepdims=True)

    def to_column(row, size):
        return jnp.broadcast_to(row, (LANES, row.shape[1])).T[:size, 0:1]

    def all_of(block, sem):
        return send(block, block, sem, sem, tp=sibling)

    def turn(i):
        return ((c // 2 + 1 + i // 2) % pairs) * 2 + (c + 1 + i) % 2

    def a_copy(l, to, frm):
        return send(
            pieces.at[l, to], spread.at[l, frm], a_send.at[l], a_recv.at[l, frm], tp=to
        )

    def q_copy(l, to, frm):
        return send(sq.at[l, frm], sq.at[l, frm], q_send.at[l], q_recv.at[l], tp=to)

    def prepare(l, p, block):
        wide = block.astype(F32)
        total = sq_sum[...]
        for lane in range(0, part, LANES):
            tile = wide[:, lane : lane + LANES]
            total = total + tile * tile
        sq_sum[...] = total
        gain = gain_ref[l : l + 1, pl.ds(pl.multiple_of(p * part, LANES), part)]
        pieces[l, p] = (wide * gain).astype(BF16)

    def hand_out(l, p):
        @pl.when(p != c)
        def _():
            a_copy(l, p, c).start()

        @pl.when(p == c)
        def _():
            spread[l, c] = pieces[l, c]

    def hand_out_squares(l):
        sq[l, c] = jnp.broadcast_to(to_row(sq_sum[...]), sq.shape[2:])
        for j in range(1, tp):
            q_copy(l, (c + j) % tp, c).start()

    def beyond(left):
        return (1 - left) * (sp - 1 - s) + left * s

    def z_copy(l, left, o, k):
        rows_k = pl.ds(k * cut, cut)
        return send(
            wo.at[l, o, g, rows_k],
            wo.at[l, o, g, rows_k],
            z_send.at[l, left],
            z_recv.at[l, o, k],
            sp=s + 1 - 2 * left,
        )

    def y_copy(l, j, o, n, k):
        rows_k = pl.ds(k * cut, cut)
        return send(
            wo.at[l, o, n, rows_k],
            wo.at[l, o, n, rows_k],
            y_send.at[l, j],
            y_recv.at[l, n],
            grp=(g + j) % grp,
        )

    def z_take(l, o, k):
        rows_k = pl.ds(k * cut, cut)
        send(
            wo.at[l, o, g, rows_k],
            wo.at[l, o, g, rows_k],
            z_send.at[l, 0],
            z_recv.at[l, o, k],
            sp=(s + 1) % sp,
        ).wait_recv()
        for j in range(1, grp):
            y_copy(l, j, o, g, k).start()

    def moment(l, left, ahead, i, k):
        if l == 0:
            table = FIRST
        else:
            table = LATER
        points = table.get((ahead, i, left), table.get((ahead, i), ("closed",) * 4))[4 * k // cuts]
        return points.split() if " " in points else (points, points)

    def fill(l, point):
        for left in range(2):
            for ahead in range(sp):
                steps = []
                for i in range(sp - ahead):
                    for k in range(cuts):
                        taken, sent_on = moment(l, left, min(ahead, 3), i, k)
                        if i > 0 and taken == point:
                            steps.append((i, k, True))
                        if ahead > 0 and sent_on == point:
                            steps.append((i, k, False))

                if steps:

                    @pl.when(beyond(left) == ahead)
                    def _():
                        for i, k, take in steps:
                            o = s + (2 * left - 1) * i
                            if take:
                                z_take(l, o, k)
                            else:
                                z_copy(l, left, o, k).start()

    def lends(l):
        return l > 0 and sp >= 4 and kept < chunks

    def sent_chunks(l, d):
        if not lends(l):
            return chunks
        return chunks - (chunks - kept) * (at_end & (d == partner)).astype(jnp.int32)

    def v_copy(l, t):
        half, q = t % 2, t // 2
        rows_q = pl.ds(pl.multiple_of((g * lots + q) * lot, lot), lot)
        return send(
            wvg.at[l, half, rows_q, pl.ds(kept * step, (chunks - kept) * step)],
            lent.at[l - 1, half, rows_q],
            v_send.at[l - 1],
            v_recv.at[l - 1, half, q],
            sp=partner,
        )

    def u_copy(l, j, t, n):
        half, q = t % 2, t // 2
        rows_q = pl.ds(pl.multiple_of((n * lots + q) * lot, lot), lot)
        return send(
            lent.at[l - 1, half, rows_q],
            lent.at[l - 1, half, rows_q],
            u_send.at[l - 1, j],
            u_recv.at[l - 1, n],
            grp=(g + j) % grp,
        )

    def lot_of(l):
        return lent.at[l - 1, pl.ds(0, 2), pl.ds(0, depth // grp)]

    def lend_out(l, first, last):
        if lends(l):

            @pl.when(at_end)
            def _():
                for t in range(first, last):
                    v_copy(l, t).start()

    def lend_in(l, first, last):
        if lends(l):

            @pl.when(at_host)
            def _():
                for t in range(first, last):
                    v_copy(l, t).wait_recv()
                    for j in range(1, grp):
                        u_copy(l, j, t, g).start()

    def place(j):
        left = (j + 2 * s // sp) % 2
        k = j // 2
        d = (1 - left) * (sp - 1 - k) + left * k
        return left, d, (1 - 2 * left) * (d - s) > 0

    def each(body):
        def one(j, carry):
            left, d, valid = place(j)

            @pl.when(valid)
            def _():
                body(j, left, d)

            return carry

        lax.fori_loop(0, 2 * (sp - 1), one, 0)

    def behind(left):
        return (1 - left) * s + left * (sp - 1 - s)

    def upstream(left):
        return behind(left) > 0

    def b_copy(l, to, frm):
        return send(
            spread.at[l, to], xs.at[l, c, frm], b_send.at[l], x_recv.at[l, c, frm], sp=to
        )

    def c_copy(l, to, d, sem):
        return send(xs.at[l, c, d], xs.at[l, c, d], sem, x_recv.at[l, c, d], tp=to)

    def relay(l, p, d):
        return send(
            xs.at[l, p, d], xs.at[l, p, d], c_relay.at[l, p], x_recv.at[l, p, d], tp=sibling
        )

    def r_copy(l, left, d, slot):
        return send(
            going.at[l, left, d, slot],
            coming.at[l, left, d, slot],
            r_send.at[l, left, slot],
            r_recv.at[l, d + 1 - left, slot],
            sp=s + 1 - 2 * left,
        )

    def h_copy(l, to, i):
        return send(
            halo_out.at[l, i], halo_in.at[l, i], h_send.at[l, i], h_recv.at[l, i], sp=to
        )

    def s_copy(l, b, to, frm):
        return send(
            stat.at[l, b, frm], stat.at[l, b, frm], s_send.at[l, b], s_recv.at[l, b], tp=to
        )

    def g_copy(l, b, to, p):
        block = acts.at[l, p, pl.ds(b * band, band)]
        return send(block, block, g_send.at[l, b], g_recv.at[l, p, b], tp=to)

    def layer_of(l):
        slots = 2 * chunks
        inner = sp == 4 and slots >= 2
        mids = 1 - at_end.astype(jnp.int32)

        def held(e):
            @pl.when(e != c)
            def _():
                a_copy(l, c, e).wait_recv()

        def scatter(j, left, d):
            held(d)
            b_copy(l, d, s).start()

        if l > 0:
            fill(l, "before")
            lend_in(l, 0, lots)
        each(scatter)
        fill(l, "scattered")
        held(s)
        xs[l, c, s] = spread[l, s]
        if lends(l):

            @pl.when(at_host)
            def _():
                xs[l, c, sp] = spread[l, partner]

        def gather(d, arriving=True):
            if arriving:
                relay(l, c, d).wait_recv()
            for j in range(1, pairs):
                c_copy(l, (c + 2 * j) % tp, d, c_send.at[l, j]).start()
            c_copy(l, sibling, d, c_send.at[l, 0]).start()

        gather(s, False)
        if inner:
            gather(place(0)[1])
            gather(place(1 + at_end.astype(jnp.int32))[1])
        else:
            each(lambda j, left, d: gather(d))
        if l == 0:
            for load in in_loads[l]:
                load.wait()

        def ready(d):
            for j in range(1, pairs):
                p = (c + 2 * j) % tp
                relay(l, p, d).wait_recv()
                relay(l, p, d).start()
            for j in range(pairs):
                relay(l, (sibling + 2 * j) % tp, d).wait_recv()

        def product(d, weight, at):
            acc = jnp.zeros((rows, step), F32)
            for p in range(tp):
                acc = acc + jnp.dot(
                    xs[l, p, d],
                    weight[p * part : (p + 1) * part, pl.ds(at, step)],
                    preferred_element_type=F32,
                )
            return acc

        def r_arrived(left, d, slot):
            send(
                going.at[l, left, d, slot],
                coming.at[l, left, d, slot],
                r_send.at[l, left, slot],
                r_recv.at[l, d + 1 - left, slot],
                sp=(s + 1) % sp,
            ).wait_recv()

        def partial(slot, left, d):
            half, i = slot % 2, slot // 2

            @pl.when(slot == 0)
            def _():
                ready(d)

            own[half] = product(d, wvg.at[l, half], pl.multiple_of(i * step, step))

            @pl.when(upstream(left))
            def _():
                r_arrived(left, d, slot)
                own[half] += coming[l, left, d, slot].astype(F32)

            going[l, left, d, slot] = own[half].astype(BF16)
            r_copy(l, left, d, slot).start()

        def turn_slot(t):
            if not inner:
                return t // slots, t % slots
            u = t - 2
            woven = ((u >= 0) & (u < 2 * slots)).astype(jnp.int32)
            aside = woven * (1 - u % 2) * mids
            k = jnp.where(woven == 1, 2 + u // 2, jnp.where(u < 0, t, t - slots))
            k = mids * k + (1 - mids) * t
            j = aside + (1 - aside) * 2 * (k // slots)
            return j, aside * (u // 2) + (1 - aside) * (k % slots)

        def advance(t, carry):
            j, slot = turn_slot(t)
            left, d, valid = place(j)

            @pl.when(valid & (slot < 2 * sent_chunks(l, d)))
            def _():
                partial(slot, left, d)

            @pl.when(t == 0)
            def _():
                if inner:
                    gather(place(2 + 2 * at_end.astype(jnp.int32))[1])
                if lends(l):

                    @pl.when(at_host)
                    def _():
                        gather(sp, False)

                lend_in(l, lots, early_lots)
                fill(l, "gathered")
                lend_out(l, early_lots, 2 * lots)

            @pl.when(t == slots - 1 + (mids * (slots - 2) if inner else 0))
            def _():
                fill(l, "turned")
                lend_in(l, early_lots, 2 * lots)

            @pl.when(t == 2 * slots - 1)
            def _():
                fill(l, "halfway")

            return carry

        lax.fori_loop(0, slots * (3 if inner else 2 * (sp - 1)), advance, 0)
        fill(l, "summed")
        ready(s)
        if lends(l):

            @pl.when(at_host)
            def _():
                ready(sp)
                for j in range(1, grp):
                    all_of(lot_of(l), u_recv.at[l - 1, (g + j) % grp]).wait_recv()

        all_of(sq.at[l, pl.ds(0, tp - 1)], q_recv.at[l]).wait_recv()
        squares = sq[l, 0]
        for p in range(1, tp):
            squares = squares + sq[l, p]
        scale = to_column(lax.rsqrt(squares[0:1] / (depth * tp) + 1e-06), rows)

        def finish(i, carry):
            at = pl.multiple_of(i * step, step)
            for half in range(2):
                slot = 2 * i + half
                own[half] = product(s, wvg.at[l, half], at)
                if lends(l):

                    @pl.when(at_host & (i >= kept))
                    def _():
                        own[half] += product(
                            sp, lent.at[l - 1, half], pl.multiple_of(at - kept * step, step)
                        )

                for left in range(2):
                    expected = upstream(left)
                    if lends(l):
                        expected = expected & jnp.logical_not(
                            at_host & (behind(left) == 1) & (i >= kept)
                        )

                    @pl.when(expected)
                    def _():
                        r_arrived(left, s, slot)
                        own[half] += coming[l, left, s, slot].astype(F32)

            glu = (own[0] * scale * jax.nn.sigmoid(own[1] * scale)).astype(BF16)
            ext[pad:, pl.ds(at, step)] = glu.astype(F32)
            halo_out[l, i] = glu[rows - pad :]

            @pl.when(s < sp - 1)
            def _():
                h_copy(l, s + 1, i).start()

            return carry

        lax.fori_loop(0, chunks, finish, 0)
        if l == 0:
            for load in small_loads:
                load.wait()
        fill(l, "finished")
        first = pad - (reach - 1)

        def halo_in_place(i, carry):
            lanes = pl.ds(pl.multiple_of(i * step, step), step)

            @pl.when(s > 0)
            def _():
                h_copy(l, (s + 1) % sp, i).wait_recv()
                ext[:pad, lanes] = halo_in[l, i].astype(F32)

            @pl.when(s == 0)
            def _():
                ext[:pad, lanes] = jnp.zeros((pad, step), F32)

            return carry

        def strip(b, i, carry):
            lanes = pl.ds(pl.multiple_of(i * LANES, LANES), LANES)
            above = first + b * band
            acc = jnp.zeros((band, LANES), F32)
            for k in range(reach):
                acc = acc + taps_ref[k, l : l + 1, lanes] * ext[above + k : above + k + band, lanes]
            conv[b * band : (b + 1) * band, lanes] = acc
            return carry

        half = stat.shape[3] // 2
        for b in reversed(range(bands)):
            if b == 0:
                lax.fori_loop(0, chunks, halo_in_place, 0)
            lax.fori_loop(0, chans // LANES, functools.partial(strip, b), 0)
            total = jnp.zeros((band, LANES), F32)
            total_sq = jnp.zeros((band, LANES), F32)
            for at in range(0, chans, LANES):
                tile = conv[b * band : (b + 1) * band, at : at + LANES]
                total = total + tile
                total_sq = total_sq + tile * tile
            stat[l, b, c] = jnp.concatenate(
                [
                    jnp.broadcast_to(to_row(t), (half, stat.shape[4]))
                    for t in (total, total_sq)
                ],
                axis=0,
            )
            for j in range(1, tp):
                s_copy(l, b, (c + j) % tp, c).start()
        fill(l, "counted")
        if l + 1 < layers:
            for load in out_loads[l + 1]:
                load.wait()
            for load in in_loads[l + 1]:
                load.wait()
            fill(l + 1, "tail")
            lend_out(l + 1, 0, early_lots)
        for b in reversed(range(bands)):
            all_of(stat.at[l, b, pl.ds(0, tp - 1)], s_recv.at[l, b]).wait_recv()
            stats = stat[l, b, 0]
            for p in range(1, tp):
                stats = stats + stat[l, b, p]
            mean = stats[0:1] / (chans * tp)
            var = stats[half : half + 1] / (chans * tp) - mean * mean
            inv = to_column(lax.rsqrt(var + 1e-05), band)
            mean = to_column(mean, band)
            here = slice(b * band, (b + 1) * band)
            for at in range(0, chans, LANES):
                lanes = slice(at, at + LANES)
                shaped = (conv[here, lanes] - mean) * inv * lng_ref[l : l + 1, lanes] + lnb_ref[
                    l : l + 1, lanes
                ]
                acts[l, c, here, lanes] = (shaped / (1.0 + jnp.exp(-shaped))).astype(BF16)
            for j in range(1, pairs):
                g_copy(l, b, (c + 2 * j) % tp, c).start()
            g_copy(l, b, sibling, c).start()
        fill(l, "closed")
        if l + 1 < layers:
            fill(l + 1, "start")
        for b in reversed(range(bands)):
            for j in range(1, pairs):
                p = (c + 2 * j) % tp
                g_copy(l, b, sibling, p).wait_recv()
                g_copy(l, b, sibling, p).start()
        for j in range(pairs):
            p = (sibling + 2 * j) % tp
            for b in range(bands):
                g_copy(l, b, sibling, p).wait_recv()
        for j in range(1, grp):
            all_of(wo.at[l, pl.ds(0, sp - 1), 0], y_recv.at[l, (g + j) % grp]).wait_recv()

        sq_sum[...] = jnp.zeros_like(sq_sum)

        def project(i, carry):
            p = turn(i)
            lanes = pl.ds(pl.multiple_of(p * part, LANES), part)
            acc = jnp.zeros((rows, part), F32)
            for e in range(tp):
                for n in range(grp):
                    acc = acc + jnp.dot(
                        acts[l, e, :, n * share : (n + 1) * share],
                        wo[l, e, n, :, lanes],
                        preferred_element_type=F32,
                    )
            before = h_ref if l == 0 else mid.at[l - 1]
            block = (before[:, lanes].astype(F32) + acc).astype(BF16)
            if l + 1 < layers:
                mid[l, :, lanes] = block
                prepare(l + 1, p, block)
                hand_out(l + 1, p)
            else:
                out_ref[:, lanes] = block
            return carry

        lax.fori_loop(0, tp, project, 0)
        if l + 1 < layers:
            hand_out_squares(l + 1)

    sq_sum[...] = jnp.zeros_like(sq_sum)
    for load in first_loads:
        load.wait()
    for p in range(tp):
        prepare(0, p, h_ref[:, p * part : (p + 1) * part])
    for load in out_loads[0]:
        load.wait()
    pl.semaphore_wait(barrier, tp + sp + grp - 3)

    def first_hand_out(i, carry):
        hand_out(0, turn(i))
        return carry

    lax.fori_loop(0, tp, first_hand_out, 0)
    fill(0, "start")
    hand_out_squares(0)
    for l in range(layers):
        layer_of(l)

    def sent(block, sem):
        all_of(block, sem).wait_send()

    def sent_some(count, most, block, sem):
        for n in range(1, most + 1):

            @pl.when(count == n)
            def _():
                sent(block(n), sem)

    for l in range(layers):
        sent(pieces.at[l, pl.ds(0, tp - 1)], a_send.at[l])
        sent(sq.at[l, pl.ds(0, tp - 1)], q_send.at[l])
        sent(spread.at[l, pl.ds(0, sp - 1)], b_send.at[l])
        for b in range(bands):
            sent(stat.at[l, b, pl.ds(0, tp - 1)], s_send.at[l, b])
            sent(acts.at[l, pl.ds(0, tp - 1), pl.ds(b * band, band)], g_send.at[l, b])

        def exchanged(n):
            for j in range(pairs):
                sent(xs.at[l, 0, pl.ds(0, n)], c_send.at[l, j])
            for j in range(1, pairs):
                sent(xs.at[l, 0, pl.ds(0, n)], c_relay.at[l, (c + 2 * j) % tp])

        if lends(l):
            for host in (False, True):

                @pl.when(at_host == host)
                def _():
                    exchanged(sp + host)

            @pl.when(at_host)
            def _():
                for j in range(1, grp):
                    sent(lot_of(l), u_send.at[l - 1, j])

            @pl.when(at_end)
            def _():
                sent(lot_of(l), v_send.at[l - 1])
        else:
            exchanged(sp)

        for left in range(2):
            for slot in range(2 * chunks):
                skipped = at_end.astype(jnp.int32) * int(lends(l) and slot >= 2 * kept)
                sent_some(
                    beyond(left) - skipped,
                    sp - 1,
                    lambda n: going.at[l, left, pl.ds(0, n), slot],
                    r_send.at[l, left, slot],
                )
            sent_some(
                (behind(left) + 1) * (beyond(left) > 0).astype(jnp.int32),
                sp - 1,
                lambda n: wo.at[l, pl.ds(0, n), 0],
                z_send.at[l, left],
            )
        for j in range(1, grp):
            sent(wo.at[l, pl.ds(0, sp - 1), 0], y_send.at[l, j])

        @pl.when(s < sp - 1)
        def _():
            for i in range(chunks):
                h_copy(l, s + 1, i).wait_send()


def fused(tokens, rms_gain, w_value, w_gate, taps, ln_gain, ln_bias, w_out):
    sp, tp, grp = (lax.axis_size(a) for a in ("sp", "tp", "grp"))
    rows, depth = tokens.shape
    padded = -(-rows // LANES) * LANES
    layers, chans, reach = w_value.shape[0], w_value.shape[2], taps.shape[1]
    part, step = depth // tp, min(2 * LANES, chans)
    slots = 2 * (chans // step)
    pad = -(-(reach - 1) // 16) * 16
    share = w_out.shape[1] // grp
    cuts = CUTS
    bands = 2 if rows % 32 == 0 and rows // 2 >= pad else 1
    vmem, dma = pltpu.VMEM, pltpu.SemaphoreType.DMA
    there = pl.BlockSpec(memory_space=pltpu.HBM)
    return pl.pallas_call(
        functools.partial(gated_conv, layers, sp, tp),
        out_shape=jax.ShapeDtypeStruct((rows, depth), BF16),
        in_specs=[there] * 8,
        out_specs=pl.BlockSpec(memory_space=pltpu.VMEM),
        scratch_shapes=[
            vmem((rows, depth), BF16),
            vmem((layers, depth), F32),
            vmem((reach, layers, chans), F32),
            vmem((layers, chans), F32),
            vmem((layers, chans), F32),
            vmem((layers, rows, depth), BF16),
            vmem((layers, 2, depth, chans), BF16),
            vmem((layers, sp, grp, share, depth), BF16),
            vmem((max(layers - 1, 1), 2, depth, chans // step // 2 * step), BF16),
            vmem((layers, tp, rows, part), BF16),
            vmem((layers, tp, rows, part), BF16),
            vmem((layers, tp, sp + 1, rows, part), BF16),
            vmem((layers, 2, sp, slots, rows, step), BF16),
            vmem((layers, 2, sp, slots, rows, step), BF16),
            vmem((2, rows, step), F32),
            vmem((layers, tp, 8, padded), F32),
            vmem((rows, LANES), F32),
            vmem((layers, bands, tp, 8, -(-rows // bands // LANES) * LANES), F32),
            vmem((layers, chans // step, pad, step), BF16),
            vmem((layers, chans // step, pad, step), BF16),
            vmem((pad + rows, chans), F32),
            vmem((rows, chans), F32),
            vmem((layers, tp, rows, chans), BF16),
            dma((5,)), dma((layers, 2)),
            dma((layers,)), dma((layers, tp)), dma((layers,)),
            dma((layers, tp // 2)), dma((layers, tp)), dma((layers, tp, sp + 1)),
            dma((layers, 2, slots)), dma((layers, sp + 1, slots)),
            dma((layers,)), dma((layers,)), dma((layers, bands)), dma((layers, bands)),
            dma((layers, chans // step)), dma((layers, chans // step)),
            dma((layers, bands)), dma((layers, tp, bands)),
            dma((layers, grp)), dma((layers, 2)), dma((layers, sp, cuts)),
            dma((layers, grp)), dma((layers, grp)),
            dma((layers,)), dma((layers, 2, LOTS)), dma((layers, grp)), dma((layers, grp)),
        ],
        compiler_params=pltpu.CompilerParams(
            collective_id=0, has_side_effects=True, vmem_limit_bytes=60 * 2**20
        ),
    )(
        tokens, rms_gain, w_value, w_gate, jnp.transpose(taps, (1, 0, 2)), ln_gain, ln_bias, w_out
    )


def fits(tokens, w_value, taps, w_out):
    sp, tp, grp = (lax.axis_size(a) for a in ("sp", "tp", "grp"))
    rows, depth = tokens.shape
    chans = w_value.shape[2]
    return (
        sp == tp
        and tp % 2 == 0
        and depth % (tp * LANES) == 0
        and chans % (LANES * grp) == 0
        and w_out.shape[1] % (16 * grp * CUTS) == 0
        and w_out.shape[1] == chans
        and depth % (16 * grp * LOTS) == 0
        and chans % min(2 * LANES, chans) == 0
        and rows % 16 == 0
        and rows >= -(-(taps.shape[1] - 1) // 16) * 16
    )


def shards(tokens, rms_gain, w_value, w_gate, taps, ln_gain, ln_bias, w_out):
    if fits(tokens, w_value, taps, w_out):
        return fused(tokens, rms_gain, w_value, w_gate, taps, ln_gain, ln_bias, w_out)
    layers = w_value.shape[0]
    tok_rows = tokens.shape[0]
    chans = w_value.shape[2]
    all_chans = chans * lax.axis_size("tp")
    reach = taps.shape[1]
    current = tokens
    for layer in range(layers):
        whole_rows = lax.all_gather(current, "tp", axis=1, tiled=True)
        normed = to_depth(norm_rows(whole_rows.astype(jnp.float32), rms_gain[layer]))
        both = jnp.concatenate([w_value[layer], w_gate[layer]], axis=1)
        both = summed(jnp.dot(normed, both, preferred_element_type=jnp.float32))
        glu = (both[:, :chans] * jax.nn.sigmoid(both[:, chans:])).astype(jnp.bfloat16)
        earlier = passed_along(glu[tok_rows - (reach - 1) :], "sp", 1)
        extended = jnp.concatenate([earlier, glu], axis=0).astype(jnp.float32)
        conv = jnp.zeros((tok_rows, chans), jnp.float32)
        for k in range(reach):
            conv = conv + taps[layer, k][None, :] * extended[k : k + tok_rows]
        total, total_sq = lax.psum((jnp.sum(conv, axis=1), jnp.sum(conv * conv, axis=1)), "tp")
        mean = total / all_chans
        var = total_sq / all_chans - mean * mean
        shaped = (conv - mean[:, None]) * lax.rsqrt(var + 1e-05)[:, None] * ln_gain[layer][
            None, :
        ] + ln_bias[layer][None, :]
        act = jax.nn.silu(shaped).astype(jnp.bfloat16)
        act_all = to_depth(lax.all_gather(act, "tp", axis=1, tiled=True))
        branch = summed(jnp.dot(act_all, w_out[layer], preferred_element_type=jnp.float32))
        current = (current.astype(jnp.float32) + branch).astype(jnp.bfloat16)
    return current


def solution(mesh):
    return jax.shard_map(
        shards,
        mesh=mesh,
        in_specs=(
            P(("grp", "sp"), "tp"),
            P(),
            P(None, "sp", "tp"),
            P(None, "sp", "tp"),
            P(None, None, "tp"),
            P(None, "tp"),
            P(None, "tp"),
            P(None, "sp", "tp"),
        ),
        out_specs=P(("grp", "sp"), "tp"),
        check_vma=False,
    )
```

```python
import functools

import jax
import jax.numpy as jnp
from jax import lax
from jax.experimental import pallas as pl
from jax.experimental.pallas import tpu as pltpu
from jax.sharding import PartitionSpec as P

LANES = 128
BF16, F32 = jnp.bfloat16, jnp.float32
LOTS = 2
CUTS = 8

FIRST = {
    (1, 0): ("start", "start", "gathered", "gathered"),
    (2, 0): ("start", "start", "scattered", "turned"),
    (3, 0): ("start", "start", "scattered", "finished"),
    (0, 1): ("gathered", "gathered", "summed", "summed"),
    (1, 1): ("gathered", "gathered", "turned summed", "summed"),
    (2, 1): ("gathered summed", "gathered finished", "gathered finished", "counted"),
    (0, 2): ("summed", "summed", "counted", "counted"),
    (1, 2): ("counted", "counted", "closed", "closed"),
}
LATER = {
    (1, 0): ("start", "start", "start", "start"),
    (2, 0): ("tail", "tail", "tail", "tail"),
    (3, 0): ("tail", "tail", "tail", "tail"),
    (0, 1): ("gathered", "gathered", "gathered", "gathered"),
    (1, 1): ("before", "before", "gathered", "gathered"),
    (2, 1): ("start", "before", "scattered", "scattered"),
    (0, 2): ("summed", "summed", "summed", "summed"),
    (1, 2, 0): ("summed", "summed", "finished", "finished"),
    (1, 2, 1): ("summed", "summed", "summed", "summed"),
    (0, 3, 0): ("counted", "counted", "counted", "closed"),
    (0, 3, 1): ("counted", "counted", "counted", "closed"),
}


def passed_along(block, axis, distance):
    devices = range(lax.axis_size(axis))
    route = [(i - distance, i) for i in devices if i - distance in devices]
    return lax.ppermute(block, axis, route)


def norm_rows(wide, gain):
    return (wide * lax.rsqrt(jnp.mean(wide * wide, axis=1, keepdims=True) + 1e-06) * gain).astype(
        jnp.bfloat16
    )


def to_depth(rows):
    return lax.all_to_all(rows, "sp", split_axis=1, concat_axis=0, tiled=True)


def summed(partial):
    sp = lax.axis_size("sp")
    rows = partial.shape[0] // sp
    parts = partial.astype(jnp.bfloat16).reshape(sp, rows, partial.shape[1])
    parts = lax.all_to_all(parts, "sp", split_axis=0, concat_axis=0, tiled=True)
    return jnp.sum(parts.astype(jnp.float32), axis=0)


def send(src, dst, send_sem, recv_sem, **where):
    return pltpu.make_async_remote_copy(
        src_ref=src,
        dst_ref=dst,
        send_sem=send_sem,
        recv_sem=recv_sem,
        device_id=where,
        device_id_type=pl.DeviceIdType.MESH,
    )


def gated_conv(
    layers, sp, tp,
    h_hbm, gain_hbm, wv_hbm, wg_hbm, taps_hbm, lng_hbm, lnb_hbm, wo_hbm, out_ref,
    h_ref, gain_ref, taps_ref, lng_ref, lnb_ref, mid,
    wvg, wo, lent, pieces, spread, xs, going, coming, own, sq, sq_sum, stat,
    halo_out, halo_in, ext, conv, acts,
    i_sem, w_sem, a_send, a_recv, b_send, c_send, c_relay, x_recv, r_send, r_recv,
    q_send, q_recv, s_send, s_recv, h_send, h_recv, g_send, g_recv,
    o_sem, z_send, z_recv, y_send, y_recv, v_send, v_recv, u_send, u_recv,
):
    s, c, g = lax.axis_index("sp"), lax.axis_index("tp"), lax.axis_index("grp")
    grp, share = wo.shape[2], wo.shape[3]
    padded = sq.shape[3]
    rows, depth = h_ref.shape
    chans = taps_ref.shape[2]
    part = depth // tp
    step = going.shape[-1]
    chunks = chans // step
    pairs = tp // 2
    sibling = c + 1 - 2 * (c % 2)
    reach = taps_ref.shape[0]
    pad = halo_in.shape[2]
    cuts = z_recv.shape[2]
    early = cuts // 2
    cut = share // cuts
    bands = stat.shape[1]
    band = rows // bands
    lots = v_recv.shape[2]
    lot = depth // (grp * lots)
    early_lots = 2 * lots
    kept = chunks - lent.shape[3] // step
    at_end = (s == 0) | (s == sp - 1)
    at_host = (s == 1) | (s == sp - 2)
    partner = (s == 0) + (sp - 2) * (s == sp - 1) + (sp - 1) * (s == sp - 2)

    first_loads = [
        pltpu.make_async_copy(h_hbm, h_ref, i_sem.at[0]),
        pltpu.make_async_copy(
            gain_hbm.at[:, pl.ds(pl.multiple_of(c * depth, LANES), depth)], gain_ref, i_sem.at[1]
        ),
    ]
    small_loads = [
        pltpu.make_async_copy(taps_hbm, taps_ref, i_sem.at[2]),
        pltpu.make_async_copy(lng_hbm, lng_ref, i_sem.at[3]),
        pltpu.make_async_copy(lnb_hbm, lnb_ref, i_sem.at[4]),
    ]
    in_loads = [
        (
            pltpu.make_async_copy(wv_hbm.at[l], wvg.at[l, 0], w_sem.at[l, 0]),
            pltpu.make_async_copy(wg_hbm.at[l], wvg.at[l, 1], w_sem.at[l, 1]),
        )
        for l in range(layers)
    ]
    out_loads = [
        [
            pltpu.make_async_copy(
                wo_hbm.at[l, pl.ds(n * share, share)], wo.at[l, s, n], o_sem.at[l, n]
            )
            for n in range(grp)
        ]
        for l in range(layers)
    ]
    for load in first_loads:
        load.start()
    for l in range(layers):
        for load in out_loads[l]:
            load.start()
        for load in in_loads[l]:
            load.start()
    for load in small_loads:
        load.start()

    barrier = pltpu.get_barrier_semaphore()
    for j in range(1, tp):
        pl.semaphore_signal(
            barrier, inc=1, device_id={"tp": (c + j) % tp}, device_id_type=pl.DeviceIdType.MESH
        )
    for j in range(1, sp):
        pl.semaphore_signal(
            barrier, inc=1, device_id={"sp": (s + j) % sp}, device_id_type=pl.DeviceIdType.MESH
        )
    for j in range(1, grp):
        pl.semaphore_signal(
            barrier, inc=1, device_id={"grp": (g + j) % grp}, device_id_type=pl.DeviceIdType.MESH
        )

    def to_row(column):
        blank = -column.shape[0] % LANES
        column = jnp.concatenate([column, jnp.zeros((blank, LANES), F32)], axis=0)
        return jnp.sum(column.T, axis=0, keepdims=True)

    def to_column(row, size):
        return jnp.broadcast_to(row, (LANES, row.shape[1])).T[:size, 0:1]

    def all_of(block, sem):
        return send(block, block, sem, sem, tp=sibling)

    def turn(i):
        return ((c // 2 + 1 + i // 2) % pairs) * 2 + (c + 1 + i) % 2

    def a_copy(l, to, frm):
        return send(
            pieces.at[l, to], spread.at[l, frm], a_send.at[l], a_recv.at[l, frm], tp=to
        )

    def q_copy(l, to, frm):
        return send(sq.at[l, frm], sq.at[l, frm], q_send.at[l], q_recv.at[l], tp=to)

    def prepare(l, p, block):
        wide = block.astype(F32)
        total = sq_sum[...]
        for lane in range(0, part, LANES):
            tile = wide[:, lane : lane + LANES]
            total = total + tile * tile
        sq_sum[...] = total
        gain = gain_ref[l : l + 1, pl.ds(pl.multiple_of(p * part, LANES), part)]
        pieces[l, p] = (wide * gain).astype(BF16)

    def hand_out(l, p):
        @pl.when(p != c)
        def _():
            a_copy(l, p, c).start()

        @pl.when(p == c)
        def _():
            spread[l, c] = pieces[l, c]

    def hand_out_squares(l):
        sq[l, c] = jnp.broadcast_to(to_row(sq_sum[...]), sq.shape[2:])
        for j in range(1, tp):
            q_copy(l, (c + j) % tp, c).start()

    def beyond(left):
        return (1 - left) * (sp - 1 - s) + left * s

    def z_copy(l, left, o, k):
        rows_k = pl.ds(k * cut, cut)
        return send(
            wo.at[l, o, g, rows_k],
            wo.at[l, o, g, rows_k],
            z_send.at[l, left],
            z_recv.at[l, o - (o > s + 1 - 2 * left).astype(jnp.int32), k],
            sp=s + 1 - 2 * left,
        )

    def y_copy(l, j, o, n, k):
        rows_k = pl.ds(k * cut, cut)
        return send(
            wo.at[l, o, n, rows_k],
            wo.at[l, o, n, rows_k],
            y_send.at[l, j],
            y_recv.at[l, n],
            grp=(g + j) % grp,
        )

    def z_take(l, o, k):
        rows_k = pl.ds(k * cut, cut)
        send(
            wo.at[l, o, g, rows_k],
            wo.at[l, o, g, rows_k],
            z_send.at[l, 0],
            z_recv.at[l, o - (o > s).astype(jnp.int32), k],
            sp=(s + 1) % sp,
        ).wait_recv()
        for j in range(1, grp):
            y_copy(l, j, o, g, k).start()

    def moment(l, left, ahead, i, k):
        if l == 0:
            table = FIRST
        else:
            table = LATER
        points = table.get((ahead, i, left), table.get((ahead, i), ("closed",) * 4))[4 * k // cuts]
        return points.split() if " " in points else (points, points)

    def fill(l, point):
        for left in range(2):
            for ahead in range(sp):
                steps = []
                for i in range(sp - ahead):
                    for k in range(cuts):
                        taken, sent_on = moment(l, left, min(ahead, 3), i, k)
                        if i > 0 and taken == point:
                            steps.append((i, k, True))
                        if ahead > 0 and sent_on == point:
                            steps.append((i, k, False))

                if steps:

                    @pl.when(beyond(left) == ahead)
                    def _():
                        for i, k, take in steps:
                            o = s + (2 * left - 1) * i
                            if take:
                                z_take(l, o, k)
                            else:
                                z_copy(l, left, o, k).start()

    def lends(l):
        return l > 0 and sp >= 4 and kept < chunks

    def sent_chunks(l, d):
        if not lends(l):
            return chunks
        return chunks - (chunks - kept) * (at_end & (d == partner)).astype(jnp.int32)

    def v_copy(l, t):
        half, q = t % 2, t // 2
        rows_q = pl.ds(pl.multiple_of((g * lots + q) * lot, lot), lot)
        return send(
            wvg.at[l, half, rows_q, pl.ds(kept * step, (chunks - kept) * step)],
            lent.at[l - 1, half, rows_q],
            v_send.at[l - 1],
            v_recv.at[l - 1, half, q],
            sp=partner,
        )

    def u_copy(l, j, t, n):
        half, q = t % 2, t // 2
        rows_q = pl.ds(pl.multiple_of((n * lots + q) * lot, lot), lot)
        return send(
            lent.at[l - 1, half, rows_q],
            lent.at[l - 1, half, rows_q],
            u_send.at[l - 1, j],
            u_recv.at[l - 1, n],
            grp=(g + j) % grp,
        )

    def lot_of(l):
        return lent.at[l - 1, pl.ds(0, 2), pl.ds(0, depth // grp)]

    def lend_out(l, first, last):
        if lends(l):

            @pl.when(at_end)
            def _():
                for t in range(first, last):
                    v_copy(l, t).start()

    def lend_in(l, first, last):
        if lends(l):

            @pl.when(at_host)
            def _():
                for t in range(first, last):
                    v_copy(l, t).wait_recv()
                    for j in range(1, grp):
                        u_copy(l, j, t, g).start()

    def place(j):
        left = (j + 2 * s // sp) % 2
        k = j // 2
        d = (1 - left) * (sp - 1 - k) + left * k
        return left, d, (1 - 2 * left) * (d - s) > 0

    def each(body):
        def one(j, carry):
            left, d, valid = place(j)

            @pl.when(valid)
            def _():
                body(j, left, d)

            return carry

        lax.fori_loop(0, 2 * (sp - 1), one, 0)

    def behind(left):
        return (1 - left) * s + left * (sp - 1 - s)

    def upstream(left):
        return behind(left) > 0

    def b_copy(l, to, frm):
        return send(
            spread.at[l, to], xs.at[l, c, frm], b_send.at[l], x_recv.at[l, c, frm], sp=to
        )

    def c_copy(l, to, d, sem):
        return send(xs.at[l, c, d], xs.at[l, c, d], sem, x_recv.at[l, c, d], tp=to)

    def relay(l, p, d):
        return send(
            xs.at[l, p, d], xs.at[l, p, d], c_relay.at[l, p], x_recv.at[l, p, d], tp=sibling
        )

    def r_copy(l, left, d, slot):
        return send(
            going.at[l, left, d, slot],
            coming.at[l, left, d, slot],
            r_send.at[l, left, slot],
            r_recv.at[l, d + 1 - left, slot],
            sp=s + 1 - 2 * left,
        )

    def h_copy(l, to, i):
        return send(
            halo_out.at[l, i], halo_in.at[l, i], h_send.at[l, i], h_recv.at[l, i], sp=to
        )

    def s_copy(l, b, to, frm):
        return send(
            stat.at[l, b, frm], stat.at[l, b, frm], s_send.at[l, b], s_recv.at[l, b], tp=to
        )

    def g_copy(l, b, to, p):
        block = acts.at[l, p, pl.ds(b * band, band)]
        return send(block, block, g_send.at[l, b], g_recv.at[l, p, b], tp=to)

    def layer_of(l):
        slots = 2 * chunks
        inner = sp == 4 and slots >= 2
        mids = 1 - at_end.astype(jnp.int32)

        def held(e):
            @pl.when(e != c)
            def _():
                a_copy(l, c, e).wait_recv()

        def scatter(j, left, d):
            held(d)
            b_copy(l, d, s).start()

        if l > 0:
            fill(l, "before")
            lend_in(l, 0, lots)
        each(scatter)
        fill(l, "scattered")
        held(s)
        xs[l, c, s] = spread[l, s]
        if lends(l):

            @pl.when(at_host)
            def _():
                xs[l, c, sp] = spread[l, partner]

        def gather(d, arriving=True):
            if arriving:
                relay(l, c, d).wait_recv()
            for j in range(1, pairs):
                c_copy(l, (c + 2 * j) % tp, d, c_send.at[l, j]).start()
            c_copy(l, sibling, d, c_send.at[l, 0]).start()

        gather(s, False)
        if inner:
            gather(place(0)[1])
            gather(place(1 + at_end.astype(jnp.int32))[1])
        else:
            each(lambda j, left, d: gather(d))
        if l == 0:
            for load in in_loads[l]:
                load.wait()

        def ready(d):
            for j in range(1, pairs):
                p = (c + 2 * j) % tp
                relay(l, p, d).wait_recv()
                relay(l, p, d).start()
            for j in range(pairs):
                relay(l, (sibling + 2 * j) % tp, d).wait_recv()

        def product(d, weight, at):
            acc = jnp.zeros((rows, step), F32)
            for p in range(tp):
                acc = acc + jnp.dot(
                    xs[l, p, d],
                    weight[p * part : (p + 1) * part, pl.ds(at, step)],
                    preferred_element_type=F32,
                )
            return acc

        def r_arrived(left, d, slot):
            send(
                going.at[l, left, d, slot],
                coming.at[l, left, d, slot],
                r_send.at[l, left, slot],
                r_recv.at[l, d + 1 - left, slot],
                sp=(s + 1) % sp,
            ).wait_recv()

        def partial(slot, left, d):
            half, i = slot % 2, slot // 2

            @pl.when(slot == 0)
            def _():
                ready(d)

            own[half] = product(d, wvg.at[l, half], pl.multiple_of(i * step, step))

            @pl.when(upstream(left))
            def _():
                r_arrived(left, d, slot)
                own[half] += coming[l, left, d, slot].astype(F32)

            going[l, left, d, slot] = own[half].astype(BF16)
            r_copy(l, left, d, slot).start()

        def turn_slot(t):
            if not inner:
                return t // slots, t % slots
            u = t - 2
            woven = ((u >= 0) & (u < 2 * slots)).astype(jnp.int32)
            aside = woven * (1 - u % 2) * mids
            k = jnp.where(woven == 1, 2 + u // 2, jnp.where(u < 0, t, t - slots))
            k = mids * k + (1 - mids) * t
            j = aside + (1 - aside) * 2 * (k // slots)
            return j, aside * (u // 2) + (1 - aside) * (k % slots)

        def advance(t, carry):
            j, slot = turn_slot(t)
            left, d, valid = place(j)

            @pl.when(valid & (slot < 2 * sent_chunks(l, d)))
            def _():
                partial(slot, left, d)

            @pl.when(t == 0)
            def _():
                if inner:
                    gather(place(2 + 2 * at_end.astype(jnp.int32))[1])
                if lends(l):

                    @pl.when(at_host)
                    def _():
                        gather(sp, False)

                lend_in(l, lots, early_lots)
                fill(l, "gathered")
                lend_out(l, early_lots, 2 * lots)

            @pl.when(t == slots - 1 + (mids * (slots - 2) if inner else 0))
            def _():
                fill(l, "turned")
                lend_in(l, early_lots, 2 * lots)

            @pl.when(t == 2 * slots - 1)
            def _():
                fill(l, "halfway")

            return carry

        lax.fori_loop(0, slots * (3 if inner else 2 * (sp - 1)), advance, 0)
        fill(l, "summed")
        ready(s)
        if lends(l):

            @pl.when(at_host)
            def _():
                ready(sp)
                for j in range(1, grp):
                    all_of(lot_of(l), u_recv.at[l - 1, (g + j) % grp]).wait_recv()

        all_of(sq.at[l, pl.ds(0, tp - 1)], q_recv.at[l]).wait_recv()
        squares = sq[l, 0]
        for p in range(1, tp):
            squares = squares + sq[l, p]
        scale = to_column(lax.rsqrt(squares[0:1] / (depth * tp) + 1e-06), rows)

        def finish(i, carry):
            at = pl.multiple_of(i * step, step)
            for half in range(2):
                slot = 2 * i + half
                own[half] = product(s, wvg.at[l, half], at)
                if lends(l):

                    @pl.when(at_host & (i >= kept))
                    def _():
                        own[half] += product(
                            sp, lent.at[l - 1, half], pl.multiple_of(at - kept * step, step)
                        )

                for left in range(2):
                    expected = upstream(left)
                    if lends(l):
                        expected = expected & jnp.logical_not(
                            at_host & (behind(left) == 1) & (i >= kept)
                        )

                    @pl.when(expected)
                    def _():
                        r_arrived(left, s, slot)
                        own[half] += coming[l, left, s, slot].astype(F32)

            glu = (own[0] * scale * jax.nn.sigmoid(own[1] * scale)).astype(BF16)
            ext[pad:, pl.ds(at, step)] = glu.astype(F32)
            halo_out[l, i] = glu[rows - pad :]

            @pl.when(s < sp - 1)
            def _():
                h_copy(l, s + 1, i).start()

            return carry

        lax.fori_loop(0, chunks, finish, 0)
        if l == 0:
            for load in small_loads:
                load.wait()
        fill(l, "finished")
        first = pad - (reach - 1)

        def halo_in_place(i, carry):
            lanes = pl.ds(pl.multiple_of(i * step, step), step)

            @pl.when(s > 0)
            def _():
                h_copy(l, (s + 1) % sp, i).wait_recv()
                ext[:pad, lanes] = halo_in[l, i].astype(F32)

            @pl.when(s == 0)
            def _():
                ext[:pad, lanes] = jnp.zeros((pad, step), F32)

            return carry

        def strip(b, i, carry):
            lanes = pl.ds(pl.multiple_of(i * LANES, LANES), LANES)
            above = first + b * band
            acc = jnp.zeros((band, LANES), F32)
            for k in range(reach):
                acc = acc + taps_ref[k, l : l + 1, lanes] * ext[above + k : above + k + band, lanes]
            conv[b * band : (b + 1) * band, lanes] = acc
            return carry

        half = stat.shape[3] // 2
        for b in reversed(range(bands)):
            if b == 0:
                lax.fori_loop(0, chunks, halo_in_place, 0)
            lax.fori_loop(0, chans // LANES, functools.partial(strip, b), 0)
            total = jnp.zeros((band, LANES), F32)
            total_sq = jnp.zeros((band, LANES), F32)
            for at in range(0, chans, LANES):
                tile = conv[b * band : (b + 1) * band, at : at + LANES]
                total = total + tile
                total_sq = total_sq + tile * tile
            stat[l, b, c] = jnp.concatenate(
                [
                    jnp.broadcast_to(to_row(t), (half, stat.shape[4]))
                    for t in (total, total_sq)
                ],
                axis=0,
            )
            for j in range(1, tp):
                s_copy(l, b, (c + j) % tp, c).start()
        fill(l, "counted")
        if l + 1 < layers:
            for load in out_loads[l + 1]:
                load.wait()
            for load in in_loads[l + 1]:
                load.wait()
            fill(l + 1, "tail")
            lend_out(l + 1, 0, early_lots)
        for b in reversed(range(bands)):
            all_of(stat.at[l, b, pl.ds(0, tp - 1)], s_recv.at[l, b]).wait_recv()
            stats = stat[l, b, 0]
            for p in range(1, tp):
                stats = stats + stat[l, b, p]
            mean = stats[0:1] / (chans * tp)
            var = stats[half : half + 1] / (chans * tp) - mean * mean
            inv = to_column(lax.rsqrt(var + 1e-05), band)
            mean = to_column(mean, band)
            here = slice(b * band, (b + 1) * band)
            for at in range(0, chans, LANES):
                lanes = slice(at, at + LANES)
                shaped = (conv[here, lanes] - mean) * inv * lng_ref[l : l + 1, lanes] + lnb_ref[
                    l : l + 1, lanes
                ]
                acts[l, c, here, lanes] = (shaped / (1.0 + jnp.exp(-shaped))).astype(BF16)
            for j in range(1, pairs):
                g_copy(l, b, (c + 2 * j) % tp, c).start()
            g_copy(l, b, sibling, c).start()
        fill(l, "closed")
        if l + 1 < layers:
            fill(l + 1, "start")
        for b in reversed(range(bands)):
            for j in range(1, pairs):
                p = (c + 2 * j) % tp
                g_copy(l, b, sibling, p).wait_recv()
                g_copy(l, b, sibling, p).start()
        for j in range(pairs):
            p = (sibling + 2 * j) % tp
            for b in range(bands):
                g_copy(l, b, sibling, p).wait_recv()
        for j in range(1, grp):
            all_of(wo.at[l, pl.ds(0, sp - 1), 0], y_recv.at[l, (g + j) % grp]).wait_recv()

        sq_sum[...] = jnp.zeros_like(sq_sum)

        def project(i, carry):
            p = turn(i)
            lanes = pl.ds(pl.multiple_of(p * part, LANES), part)
            acc = jnp.zeros((rows, part), F32)
            for e in range(tp):
                for n in range(grp):
                    acc = acc + jnp.dot(
                        acts[l, e, :, n * share : (n + 1) * share],
                        wo[l, e, n, :, lanes],
                        preferred_element_type=F32,
                    )
            before = h_ref if l == 0 else mid.at[l - 1]
            block = (before[:, lanes].astype(F32) + acc).astype(BF16)
            if l + 1 < layers:
                mid[l, :, lanes] = block
                prepare(l + 1, p, block)
                hand_out(l + 1, p)
            else:
                out_ref[:, lanes] = block
            return carry

        lax.fori_loop(0, tp, project, 0)
        if l + 1 < layers:
            hand_out_squares(l + 1)

    sq_sum[...] = jnp.zeros_like(sq_sum)
    for load in first_loads:
        load.wait()
    for p in range(tp):
        prepare(0, p, h_ref[:, p * part : (p + 1) * part])
    for load in out_loads[0]:
        load.wait()
    pl.semaphore_wait(barrier, tp + sp + grp - 3)

    def first_hand_out(i, carry):
        hand_out(0, turn(i))
        return carry

    lax.fori_loop(0, tp, first_hand_out, 0)
    fill(0, "start")
    hand_out_squares(0)
    for l in range(layers):
        layer_of(l)

    def sent(block, sem):
        all_of(block, sem).wait_send()

    def sent_some(count, most, block, sem):
        for n in range(1, most + 1):

            @pl.when(count == n)
            def _():
                sent(block(n), sem)

    for l in range(layers):
        sent(pieces.at[l, pl.ds(0, tp - 1)], a_send.at[l])
        sent(sq.at[l, pl.ds(0, tp - 1)], q_send.at[l])
        sent(spread.at[l, pl.ds(0, sp - 1)], b_send.at[l])
        for b in range(bands):
            sent(stat.at[l, b, pl.ds(0, tp - 1)], s_send.at[l, b])
            sent(acts.at[l, pl.ds(0, tp - 1), pl.ds(b * band, band)], g_send.at[l, b])

        def exchanged(n):
            for j in range(pairs):
                sent(xs.at[l, 0, pl.ds(0, n)], c_send.at[l, j])
            for j in range(1, pairs):
                sent(xs.at[l, 0, pl.ds(0, n)], c_relay.at[l, (c + 2 * j) % tp])

        if lends(l):
            for host in (False, True):

                @pl.when(at_host == host)
                def _():
                    exchanged(sp + host)

            @pl.when(at_host)
            def _():
                for j in range(1, grp):
                    sent(lot_of(l), u_send.at[l - 1, j])

            @pl.when(at_end)
            def _():
                sent(lot_of(l), v_send.at[l - 1])
        else:
            exchanged(sp)

        for left in range(2):
            for slot in range(2 * chunks):
                skipped = at_end.astype(jnp.int32) * int(lends(l) and slot >= 2 * kept)
                sent_some(
                    beyond(left) - skipped,
                    sp - 1,
                    lambda n: going.at[l, left, pl.ds(0, n), slot],
                    r_send.at[l, left, slot],
                )
            sent_some(
                (behind(left) + 1) * (beyond(left) > 0).astype(jnp.int32),
                sp - 1,
                lambda n: wo.at[l, pl.ds(0, n), 0],
                z_send.at[l, left],
            )
        for j in range(1, grp):
            sent(wo.at[l, pl.ds(0, sp - 1), 0], y_send.at[l, j])

        @pl.when(s < sp - 1)
        def _():
            for i in range(chunks):
                h_copy(l, s + 1, i).wait_send()


def fused(tokens, rms_gain, w_value, w_gate, taps, ln_gain, ln_bias, w_out):
    sp, tp, grp = (lax.axis_size(a) for a in ("sp", "tp", "grp"))
    rows, depth = tokens.shape
    padded = -(-rows // LANES) * LANES
    layers, chans, reach = w_value.shape[0], w_value.shape[2], taps.shape[1]
    part, step = depth // tp, min(2 * LANES, chans)
    slots = 2 * (chans // step)
    pad = -(-(reach - 1) // 16) * 16
    share = w_out.shape[1] // grp
    cuts = CUTS
    bands = 2 if rows % 32 == 0 and rows // 2 >= pad else 1
    vmem, dma = pltpu.VMEM, pltpu.SemaphoreType.DMA
    there = pl.BlockSpec(memory_space=pltpu.HBM)
    return pl.pallas_call(
        functools.partial(gated_conv, layers, sp, tp),
        out_shape=jax.ShapeDtypeStruct((rows, depth), BF16),
        in_specs=[there] * 8,
        out_specs=pl.BlockSpec(memory_space=pltpu.VMEM),
        scratch_shapes=[
            vmem((rows, depth), BF16),
            vmem((layers, depth), F32),
            vmem((reach, layers, chans), F32),
            vmem((layers, chans), F32),
            vmem((layers, chans), F32),
            vmem((layers, rows, depth), BF16),
            vmem((layers, 2, depth, chans), BF16),
            vmem((layers, sp, grp, share, depth), BF16),
            vmem((max(layers - 1, 1), 2, depth, chans // step // 2 * step), BF16),
            vmem((layers, tp, rows, part), BF16),
            vmem((layers, tp, rows, part), BF16),
            vmem((layers, tp, sp + 1, rows, part), BF16),
            vmem((layers, 2, sp, slots, rows, step), BF16),
            vmem((layers, 2, sp, slots, rows, step), BF16),
            vmem((2, rows, step), F32),
            vmem((layers, tp, 8, padded), F32),
            vmem((rows, LANES), F32),
            vmem((layers, bands, tp, 8, -(-rows // bands // LANES) * LANES), F32),
            vmem((layers, chans // step, pad, step), BF16),
            vmem((layers, chans // step, pad, step), BF16),
            vmem((pad + rows, chans), F32),
            vmem((rows, chans), F32),
            vmem((layers, tp, rows, chans), BF16),
            dma((5,)), dma((layers, 2)),
            dma((layers,)), dma((layers, tp)), dma((layers,)),
            dma((layers, tp // 2)), dma((layers, tp)), dma((layers, tp, sp + 1)),
            dma((layers, 2, slots)), dma((layers, sp + 1, slots)),
            dma((layers,)), dma((layers,)), dma((layers, bands)), dma((layers, bands)),
            dma((layers, chans // step)), dma((layers, chans // step)),
            dma((layers, bands)), dma((layers, tp, bands)),
            dma((layers, grp)), dma((layers, 2)), dma((layers, sp - 1, cuts)),
            dma((layers, grp)), dma((layers, grp)),
            dma((layers,)), dma((layers, 2, LOTS)), dma((layers, grp)), dma((layers, grp)),
        ],
        compiler_params=pltpu.CompilerParams(
            collective_id=0, has_side_effects=True, vmem_limit_bytes=60 * 2**20
        ),
    )(
        tokens, rms_gain, w_value, w_gate, jnp.transpose(taps, (1, 0, 2)), ln_gain, ln_bias, w_out
    )


def fits(tokens, w_value, taps, w_out):
    sp, tp, grp = (lax.axis_size(a) for a in ("sp", "tp", "grp"))
    rows, depth = tokens.shape
    chans = w_value.shape[2]
    return (
        sp == tp
        and tp % 2 == 0
        and depth % (tp * LANES) == 0
        and chans % (LANES * grp) == 0
        and w_out.shape[1] % (16 * grp * CUTS) == 0
        and w_out.shape[1] == chans
        and depth % (16 * grp * LOTS) == 0
        and chans % min(2 * LANES, chans) == 0
        and rows % 16 == 0
        and rows >= -(-(taps.shape[1] - 1) // 16) * 16
    )


def shards(tokens, rms_gain, w_value, w_gate, taps, ln_gain, ln_bias, w_out):
    if fits(tokens, w_value, taps, w_out):
        return fused(tokens, rms_gain, w_value, w_gate, taps, ln_gain, ln_bias, w_out)
    layers = w_value.shape[0]
    tok_rows = tokens.shape[0]
    chans = w_value.shape[2]
    all_chans = chans * lax.axis_size("tp")
    reach = taps.shape[1]
    current = tokens
    for layer in range(layers):
        whole_rows = lax.all_gather(current, "tp", axis=1, tiled=True)
        normed = to_depth(norm_rows(whole_rows.astype(jnp.float32), rms_gain[layer]))
        both = jnp.concatenate([w_value[layer], w_gate[layer]], axis=1)
        both = summed(jnp.dot(normed, both, preferred_element_type=jnp.float32))
        glu = (both[:, :chans] * jax.nn.sigmoid(both[:, chans:])).astype(jnp.bfloat16)
        earlier = passed_along(glu[tok_rows - (reach - 1) :], "sp", 1)
        extended = jnp.concatenate([earlier, glu], axis=0).astype(jnp.float32)
        conv = jnp.zeros((tok_rows, chans), jnp.float32)
        for k in range(reach):
            conv = conv + taps[layer, k][None, :] * extended[k : k + tok_rows]
        total, total_sq = lax.psum((jnp.sum(conv, axis=1), jnp.sum(conv * conv, axis=1)), "tp")
        mean = total / all_chans
        var = total_sq / all_chans - mean * mean
        shaped = (conv - mean[:, None]) * lax.rsqrt(var + 1e-05)[:, None] * ln_gain[layer][
            None, :
        ] + ln_bias[layer][None, :]
        act = jax.nn.silu(shaped).astype(jnp.bfloat16)
        act_all = to_depth(lax.all_gather(act, "tp", axis=1, tiled=True))
        branch = summed(jnp.dot(act_all, w_out[layer], preferred_element_type=jnp.float32))
        current = (current.astype(jnp.float32) + branch).astype(jnp.bfloat16)
    return current


def solution(mesh):
    return jax.shard_map(
        shards,
        mesh=mesh,
        in_specs=(
            P(("grp", "sp"), "tp"),
            P(),
            P(None, "sp", "tp"),
            P(None, "sp", "tp"),
            P(None, None, "tp"),
            P(None, "tp"),
            P(None, "tp"),
            P(None, "sp", "tp"),
        ),
        out_specs=P(("grp", "sp"), "tp"),
        check_vma=False,
    )
```
